128 devices in a mesh: sp: 32 (over z, y, core), tp: 4 (over x).
Axes of the slice: x: 4, y: 4, z: 4, core: 2. Of those that a mesh axis runs over, the one named last changes fastest.
Arguments:
- tokens: bfloat16 [4096, 6, 2048], P(('sp', 'tp')), may hold values from -6 to 6
- norm_gain: float32 [2048], replicated, may hold values from 0.1 to 1.9
- w_query: bfloat16 [3, 2048, 1024], P(None, 'sp', 'tp'), may hold values from -0.125 to 0.125
- w_key: bfloat16 [3, 2048, 1024], P(None, 'sp', 'tp'), may hold values from -0.125 to 0.125
- w_value: bfloat16 [3, 2048, 1024], P(None, 'sp', 'tp'), may hold values from -0.125 to 0.125
- w_out: bfloat16 [1024, 2048], P('tp', 'sp'), may hold values from -0.1875 to 0.1875
Outputs:
- mixed: bfloat16 [4096, 6, 2048], P(('sp', 'tp'))
- log_weight: float32 [4096, 6, 8], P('sp', None, 'tp')
The draws below stay inside these ranges and needn't reach their ends.
All inputs are finite; a program needn't handle non-finite values.
Results may differ from the reference program's by a relative error of at most 0.015.
Values may be sent and summed in bfloat16 or wider, within the bound.
A program may use at most 128 MiB of HBM per device.

```python
import jax
import jax.numpy as jnp
from jax import lax

WIDTH = 2048
GROUPS = 3
HEADS = 8
HEAD_WIDTH = 128
STEPS = 24
DILATION_MIDDLE = 4
DILATION_WIDE = 16
BATCH = 6
LENGTH = 4096


def shard_levels(own_key, dims, pieces, least, high):
    def one(dim, blocks):
        draws = jax.random.uniform(jax.random.fold_in(jax.random.fold_in(own_key, 6), dim), (blocks,), jnp.float32, least / len(pieces), high / len(pieces))
        return jnp.repeat(jnp.exp(draws), dims[dim] // blocks).reshape((-1,) + (1,) * (len(dims) - dim - 1))

    factor_of = one(*pieces[0])
    for cut in pieces[1:]:
        factor_of = factor_of * one(*cut)
    return factor_of


def normal_values(rng, dims, spread, limit, cuts=(), kind=jnp.bfloat16):
    array = jax.random.normal(rng, dims, jnp.float32) * spread
    if len(cuts) > 0:
        array = shard_levels(rng, dims, cuts, -0.22, 0.18) * array
    return jnp.clip(array, min=-limit, max=limit).astype(kind)


def setup_inputs(seed: int = 0) -> dict:
    splits = jax.random.split(jax.random.key(seed), 7)
    tokens = normal_values(splits[0], (LENGTH, BATCH, WIDTH), 1.0, 6.0, ((0, 128),))
    norm_gain = jnp.clip(1.0 + 0.18 * jax.random.normal(splits[1], (WIDTH,), jnp.float32), 0.1, 1.9)
    w_query = normal_values(splits[2], (GROUPS, WIDTH, HEADS * HEAD_WIDTH), WIDTH ** -0.5, 0.125, ((1, 32), (2, 4)))
    w_key = normal_values(splits[3], (GROUPS, WIDTH, HEADS * HEAD_WIDTH), WIDTH ** -0.5, 0.125, ((1, 32), (2, 4)))
    w_value = normal_values(splits[4], (GROUPS, WIDTH, HEADS * HEAD_WIDTH), WIDTH ** -0.5, 0.125, ((1, 32), (2, 4)))
    w_out = normal_values(splits[5], (HEADS * HEAD_WIDTH, WIDTH), (HEADS * HEAD_WIDTH) ** -0.5, 0.1875, ((0, 4), (1, 32)))
    return dict(tokens=tokens, norm_gain=norm_gain, w_query=w_query, w_key=w_key, w_value=w_value, w_out=w_out)


epsilon = 1e-06

def rms_normed(values, gain):
    widened = values.astype(jnp.float32)
    scaled = widened * lax.rsqrt(lax.optimization_barrier(jnp.mean(widened * widened, axis=-1, keepdims=True)) + epsilon)
    return (scaled * gain.astype(jnp.float32)).astype(jnp.bfloat16)

def reference(tokens, norm_gain, w_query, w_key, w_value, w_out):
    seq_count, batch_count, width_count = tokens.shape
    normed = rms_normed(tokens, norm_gain)
    flat_rows = normed.reshape(seq_count * batch_count, width_count)
    positions = jnp.arange(seq_count, dtype=jnp.int32)
    scale = 1.0 / HEAD_WIDTH ** 0.5
    group_logs = []
    group_outs = []
    for group_index, dilation in enumerate((1, DILATION_MIDDLE, DILATION_WIDE)):

        def project(weight):
            product = jnp.dot(flat_rows, weight[group_index], preferred_element_type=jnp.float32)
            return product.astype(jnp.bfloat16).reshape(seq_count, batch_count, HEADS, HEAD_WIDTH).astype(jnp.float32)
        queries = project(w_query)
        keys = project(w_key)
        values = project(w_value)
        score_list = []
        for lag_index in range(STEPS + 1):
            offset = lag_index * dilation
            moved = jnp.pad(keys, ((offset, 0), (0, 0), (0, 0), (0, 0)))[:seq_count]
            score = jnp.einsum('sbhe,sbhe->sbh', queries, moved, precision=lax.Precision.HIGHEST) * scale
            score_list.append(jnp.where((positions >= offset)[:, None, None], score, jnp.float32(-1e+30)))
        scores = jnp.stack(score_list)
        peak = lax.optimization_barrier(jnp.max(scores, axis=0))
        lifted = jnp.exp(scores - peak[None])
        totals = lax.optimization_barrier(jnp.sum(lifted, axis=0))
        group_logs.append(peak + jnp.log(totals))
        probs = (lifted / totals[None]).astype(jnp.bfloat16).astype(jnp.float32)
        accumulated = jnp.zeros((seq_count, batch_count, HEADS, HEAD_WIDTH), jnp.float32)
        for lag_index in range(STEPS + 1):
            offset = lag_index * dilation
            moved = jnp.pad(values, ((offset, 0), (0, 0), (0, 0), (0, 0)))[:seq_count]
            accumulated = accumulated + probs[lag_index][..., None] * moved
        group_outs.append(accumulated.astype(jnp.bfloat16))
    stacked_logs = jnp.stack(group_logs)
    top_log = lax.optimization_barrier(jnp.max(stacked_logs, axis=0))
    log_weight = top_log + jnp.log(lax.optimization_barrier(jnp.sum(jnp.exp(stacked_logs - top_log[None]), axis=0)))
    shares = jax.nn.softmax(stacked_logs, axis=0)
    outputs = jnp.stack(group_outs).astype(jnp.float32)
    combined = lax.optimization_barrier(jnp.sum(shares[..., None] * outputs, axis=0)).astype(jnp.bfloat16)
    combined = combined.reshape(seq_count * batch_count, HEADS * HEAD_WIDTH)
    mixed = jnp.dot(combined, w_out, preferred_element_type=jnp.float32).astype(jnp.bfloat16)
    return (mixed.reshape(seq_count, batch_count, width_count), log_weight)
```

```python
import functools
import math

import jax
import jax.numpy as jnp
from jax import lax
from jax.experimental import pallas as pl
from jax.experimental.pallas import tpu as pltpu
from jax.sharding import PartitionSpec as P

GROUPS = 3
HEADS = 8
HEAD_WIDTH = 128
STEPS = 24
DILATION_MIDDLE = 4
DILATION_WIDE = 16
WIDTH = 2048
BATCH = 6
SHARE = BATCH // 2
ROWS = 512
BACK = (128, 128, 384)
USED = (32, 96, 384)
WINDOW = (256, 256, 512)
KEYS = sum(WINDOW)
BLOCK = 128
PIECE = 64
COLUMNS = 10 * HEAD_WIDTH
ABSENT = -1e30

epsilon = 1e-06
MESH = pl.DeviceIdType.MESH


def rms_normed(values, gain):
    widened = values.astype(jnp.float32)
    scaled = widened * lax.rsqrt(jnp.mean(widened * widened, axis=-1, keepdims=True) + epsilon)
    return (scaled * gain.astype(jnp.float32)).astype(jnp.bfloat16)


def dot(a, b):
    return lax.dot_general(a, b, (((1,), (0,)), ((), ())), preferred_element_type=jnp.float32)


def dot_t(a, b):
    return lax.dot_general(a, b, (((1,), (1,)), ((), ())), preferred_element_type=jnp.float32)


def kernel(
    normed, piece, out, logs,
    toks, weights, whole_out, queries, near, middle, wide, bias, combined, arrived,
    log_rows, own_sem, send_sem, recv_sem,
):
    s, x = lax.axis_index("sp"), lax.axis_index("tp")
    core, chip = lax.rem(s, 2), lax.div(s, 2)
    y, z = lax.rem(chip, 4), lax.div(chip, 4)

    def turn(value, by):
        return lax.rem(value + (by + 4), 4)

    def spot(y_at, z_at, core_at):
        return (z_at * 4 + y_at) * 2 + core_at

    yp, ym, zp, zm, xp, xm = (turn(v, d) for v in (y, z, x) for d in (1, -1))
    line = lax.rem(y, 2)
    pair_y = y + 1 - 2 * line
    share = lax.rem(lax.div(y + 1, 2), 2)
    other = 1 - core
    partner = (spot(y, z, other), x)
    y_plus, y_minus = (spot(yp, z, core), x), (spot(ym, z, core), x)
    z_plus, z_minus = (spot(y, zp, core), x), (spot(y, zm, core), x)
    x_plus, x_minus = (s, xp), (s, xm)
    upper = lax.div(y, 2)
    later = (spot(3 - y, turn(z, upper), core), x)
    corner = (spot(3 - y, turn(z, 2 * upper - 1), core), x)
    across = (spot(turn(pair_y, 2), z, core), x)
    head = 2 * x + core

    crowd = []
    for flip_line in (0, 1):
        for flip_core in (0, 1):
            for step in range(4):
                if flip_line or flip_core or step:
                    y_at = pair_y if flip_line else y
                    core_at = other if flip_core else core
                    crowd.append((flip_line, flip_core, step, (spot(y_at, z, core_at), turn(x, step))))
    far_y = (spot(turn(y, 2 * line - 1), z, core), x)
    greeted = [c[3] for c in crowd] + [far_y, z_plus, z_minus, corner]

    barrier = pltpu.get_barrier_semaphore()
    for device in greeted:
        pl.semaphore_signal(barrier, inc=1, device_id=device, device_id_type=MESH)

    started = []

    class Transfer:
        def __init__(self):
            self.index = len(started)
            started.append(self)

        def start(self, src, dst, device):
            self.copy = pltpu.make_async_remote_copy(
                src_ref=src, dst_ref=dst, send_sem=send_sem.at[self.index],
                recv_sem=recv_sem.at[self.index], device_id=device, device_id_type=MESH,
            )
            self.copy.start()
            return self

        def arrive(self):
            self.copy.wait_recv()

    def send(src, dst, device):
        return Transfer().start(src, dst, device)

    def weight_rows(s_at, half=None):
        at, count = s_at * PIECE, PIECE
        if half is not None:
            at, count = at + half * (PIECE // 2), PIECE // 2
        return weights.at[pl.ds(pl.multiple_of(at, 32), count), :]

    def token_rows(line_at, core_at, x_at):
        at = line_at * 256 + core_at * 128 + x_at * 32
        return toks.at[:, pl.ds(pl.multiple_of(at, 32), 32), :]

    mine_w = pltpu.make_async_copy(piece.at[core], weight_rows(s), own_sem.at[0])
    mine_t = pltpu.make_async_copy(
        normed.at[pl.ds(share * SHARE, SHARE)], token_rows(line, core, x), own_sem.at[1]
    )
    mine_w.start()
    mine_t.start()

    pl.semaphore_wait(barrier, len(greeted))

    swap = send(piece.at[other], weight_rows(s), partner)
    give = send(
        normed.at[pl.ds((1 - share) * SHARE, SHARE)],
        token_rows(line, core, x),
        (spot(pair_y, z, core), x),
    )
    mine_w.wait()

    class Ring:
        def __init__(self, rows_of, plus, minus):
            self.rows_of, self.plus, self.minus = rows_of, plus, minus
            rows = rows_of(0, None)
            self.up = send(rows, rows, plus)
            self.down = send(rows, rows, minus)

        def onward_up(self):
            self.up.arrive()
            rows = self.rows_of(-1, 0)
            self.far_up = send(rows, rows, self.plus)

        def onward_down(self):
            self.down.arrive()
            rows = self.rows_of(1, 1)
            self.far_down = send(rows, rows, self.minus)

        def onward(self):
            self.onward_up()
            self.onward_down()

        def far(self):
            self.far_up.arrive()
            self.far_down.arrive()

    def y_ring(dz, core_at):
        return Ring(
            lambda step, half: weight_rows(spot(turn(y, step), turn(z, dz), core_at), half),
            y_plus, y_minus,
        )

    def z_ring(dy, core_at):
        return Ring(
            lambda step, half: weight_rows(spot(turn(y, dy), turn(z, step), core_at), half),
            z_plus, z_minus,
        )

    own_first = y_ring(0, core)
    own_second = {0: z_ring(0, core)}
    mine_t.wait()
    first = token_rows(line, core, x)
    tok_up = [send(first, first, x_plus)]
    tok_down = [send(first, first, x_minus)]
    tok_swap = [send(first, first, partner)]
    swap.arrive()
    their_first = z_ring(0, other)
    their_second = {0: y_ring(0, other)}

    near[:, :, : BACK[0] - USED[0], :] = jnp.zeros((2, SHARE, BACK[0] - USED[0], HEAD_WIDTH), jnp.bfloat16)
    middle[:, :, : BACK[1] - USED[1], :] = jnp.zeros((2, SHARE, BACK[1] - USED[1], HEAD_WIDTH), jnp.bfloat16)
    log_rows[...] = jnp.zeros_like(log_rows)
    left = 0
    for back, window, dilation in zip(BACK, WINDOW, (1, DILATION_MIDDLE, DILATION_WIDE)):
        query_at = lax.broadcasted_iota(jnp.int32, (BLOCK, window), 0)
        key_at = lax.broadcasted_iota(jnp.int32, (BLOCK, window), 1)
        lag = query_at + back - key_at
        allowed = (lag >= 0) & (lag <= STEPS * dilation) & ((lag & (dilation - 1)) == 0)
        bias[:, left : left + window] = jnp.where(allowed, jnp.float32(0), jnp.float32(ABSENT))
        left += window

    own_first.onward()
    own_second[-1] = z_ring(-1, core)
    own_second[1] = z_ring(1, core)
    own_second[0].onward()
    their_first.onward()
    their_second[-1] = y_ring(-1, other)
    their_second[1] = y_ring(1, other)
    their_second[0].onward()

    give.arrive()
    second = token_rows(1 - line, core, x)
    tok_up.append(send(second, second, x_plus))
    tok_down.append(send(second, second, x_minus))
    tok_swap.append(send(second, second, partner))
    tok_up[0].arrive()
    rows = token_rows(line, core, xm)
    tok_far_up = send(rows, rows, x_plus)
    tok_swap.append(send(rows, rows, partner))
    tok_down[0].arrive()
    rows = token_rows(line, core, xp)
    tok_swap.append(send(rows, rows, partner))

    own_first.far()
    own_second[2] = z_ring(2, core)
    their_first.far()
    their_second[2] = y_ring(2, other)
    for step in (-1, 1):
        own_second[step].onward()
        their_second[step].onward()

    tok_down[1].arrive()
    rows = token_rows(1 - line, core, xp)
    tok_far_down = send(rows, rows, x_minus)
    tok_swap.append(send(rows, rows, partner))
    tok_up[1].arrive()
    rows = token_rows(1 - line, core, xm)
    tok_swap.append(send(rows, rows, partner))

    own_second[2].onward()
    their_second[2].onward()
    for step in (0, -1, 1, 2):
        own_second[step].far()
        their_second[step].far()
    tok_far_up.arrive()
    rows = token_rows(line, core, turn(x, 2))
    tok_swap.append(send(rows, rows, partner))
    tok_far_down.arrive()
    rows = token_rows(1 - line, core, turn(x, 2))
    tok_swap.append(send(rows, rows, partner))

    def head_columns(x_at, core_at, half=None):
        lanes = pl.ds(pl.multiple_of((2 * x_at + core_at) * HEAD_WIDTH, HEAD_WIDTH), HEAD_WIDTH)
        if half is None:
            return whole_out.at[:, lanes]
        return whole_out.at[pl.ds(half * (WIDTH // 2), WIDTH // 2), lanes]

    out_rows = weights.at[:, 9 * HEAD_WIDTH :]
    mine_o = head_columns(x, core)
    out_up = send(out_rows, mine_o, x_plus)
    out_down = send(out_rows, mine_o, x_minus)
    out_swap = [send(out_rows, mine_o, partner)]
    whole_out[:, pl.ds(pl.multiple_of(head * HEAD_WIDTH, HEAD_WIDTH), HEAD_WIDTH)] = weights[:, 9 * HEAD_WIDTH :]

    for copy in tok_swap:
        copy.arrive()

    def project(left, width, b):
        return dot(toks[b], weights[:, left : left + width]).astype(jnp.bfloat16)

    halo = []
    for place, keys in enumerate((wide, middle, near)):
        back, used = BACK[2 - place], USED[2 - place]

        def fill(b, carry, keys=keys, back=back, place=place):
            both = project(place * 2 * HEAD_WIDTH, 2 * HEAD_WIDTH, b)
            keys[0, b, back:, :] = both[:, :HEAD_WIDTH]
            keys[1, b, back:, :] = both[:, HEAD_WIDTH:]
            return carry

        lax.fori_loop(0, SHARE, fill, 0)
        halo.append(
            send(
                keys.at[:, :, back + ROWS - used :, :],
                keys.at[:, :, back - used : back, :],
                later,
            )
        )

    def ask(b, carry):
        both = project(6 * HEAD_WIDTH, 2 * HEAD_WIDTH, b)
        queries[2, b] = both[:, :HEAD_WIDTH]
        queries[1, b] = both[:, HEAD_WIDTH:]
        queries[0, b] = project(8 * HEAD_WIDTH, HEAD_WIDTH, b)
        return carry

    lax.fori_loop(0, SHARE, ask, 0)

    out_up.arrive()
    rows = head_columns(xm, core, 0)
    out_far_up = send(rows, rows, x_plus)
    rows = head_columns(xm, core)
    out_swap.append(send(rows, rows, partner))
    out_down.arrive()
    rows = head_columns(xp, core, 1)
    out_far_down = send(rows, rows, x_minus)
    rows = head_columns(xp, core)
    out_swap.append(send(rows, rows, partner))

    for copy in halo:
        copy.arrive()

    factor = math.log2(math.e) / math.sqrt(HEAD_WIDTH)
    start_at = (z * 2 + upper) * ROWS

    def attend(index, carry):
        b, block = lax.div(index, 4), lax.rem(index, 4)
        at = pl.multiple_of(block * BLOCK, BLOCK)
        scores, left = [], 0
        for group, keys in enumerate((near, middle, wide)):
            window = WINDOW[group]
            score = dot_t(queries[group, b, pl.ds(at, BLOCK), :], keys[0, b, pl.ds(at, window), :])
            key_at = lax.broadcasted_iota(jnp.int32, (1, window), 1) + (start_at + at - BACK[group])
            edge = jnp.where(key_at >= 0, jnp.float32(0), jnp.float32(ABSENT))
            scores.append(score * factor + (bias[:, left : left + window] + edge))
            left += window
        peak = functools.reduce(
            jnp.maximum, [jnp.max(score, axis=1, keepdims=True) for score in scores]
        )
        total, mixed = 0.0, 0.0
        for group, keys in enumerate((near, middle, wide)):
            lifted = jnp.exp2(scores[group] - peak)
            total = total + jnp.sum(lifted, axis=1, keepdims=True)
            mixed = mixed + dot(lifted.astype(jnp.bfloat16), keys[1, b, pl.ds(at, WINDOW[group]), :])
        combined[b, pl.ds(at, BLOCK), :] = (mixed / total).astype(jnp.bfloat16)
        log = (peak + jnp.log2(total)) * math.log(2.0)
        log_rows[block, pl.ds(b, 1), :] = jnp.transpose(
            jnp.broadcast_to(log, (BLOCK, BLOCK))
        )[0:1, :]
        return carry

    lax.fori_loop(0, SHARE * 4, attend, 0)

    lanes = pl.ds(pl.multiple_of(head * HEAD_WIDTH, HEAD_WIDTH), HEAD_WIDTH)
    mine = arrived.at[pl.ds(share * SHARE, SHARE), :, lanes]

    def rows_for(line_at, core_at, x_at):
        return pl.ds(pl.multiple_of(line_at * 256 + core_at * 128 + x_at * 32, 32), 32)

    exchange = []
    for flip_line, flip_core, step, device in crowd:
        line_at = 1 - line if flip_line else line
        core_at = other if flip_core else core
        exchange.append(
            send(combined.at[:, rows_for(line_at, core_at, turn(x, step)), :], mine, device)
        )
        if step == 0:
            exchange.append(send(log_rows.at[line_at * 2 + core_at], logs.at[core, share], device))
    arrived[pl.ds(share * SHARE, SHARE), :, lanes] = combined[:, rows_for(line, core, x), :]
    logs[core, share] = log_rows[line * 2 + core]

    out_far_up.arrive()
    rows = head_columns(turn(x, 2), core, 0)
    out_swap.append(send(rows, rows, partner))
    out_far_down.arrive()
    rows = head_columns(turn(x, 2), core, 1)
    out_swap.append(send(rows, rows, partner))
    for copy in out_swap + exchange:
        copy.arrive()

    to_row = lax.broadcasted_iota(jnp.int32, (256, 192), 0)
    from_row = lax.broadcasted_iota(jnp.int32, (256, 192), 1)
    chosen = ((from_row & 31) == (to_row >> 3)) & ((from_row >> 5) == (to_row & 7))
    order = jnp.where(chosen, jnp.float32(1), jnp.float32(0)).astype(jnp.bfloat16)
    ordered = dot(order, arrived[...].reshape(192, HEADS * HEAD_WIDTH)).astype(jnp.bfloat16)
    for tile in range(8):
        part = dot_t(ordered, whole_out[tile * 256 : (tile + 1) * 256, :])
        part = part.reshape(32, 8, 256)[:, :BATCH, :]
        out[:, :, tile * 256 : (tile + 1) * 256] = part.astype(jnp.bfloat16)

    for transfer in started:
        transfer.copy.wait_send()


TRANSFERS = 100


def shards(tokens, norm_gain, w_query, w_key, w_value, w_out):
    normed = jnp.transpose(rms_normed(tokens, norm_gain), (1, 0, 2))
    turned = jnp.transpose(w_out)
    halves = []
    for core in range(2):
        lanes = slice(core * HEAD_WIDTH, (core + 1) * HEAD_WIDTH)
        parts = []
        for group in (2, 1, 0):
            parts += [w_key[group, :, lanes], w_value[group, :, lanes]]
        parts += [w_query[group, :, lanes] for group in (2, 1, 0)]
        halves.append(jnp.concatenate(parts + [turned[:, lanes]], axis=1))
    piece = jnp.stack(halves)

    bf16, f32 = jnp.bfloat16, jnp.float32
    mixed, logs = pl.pallas_call(
        kernel,
        out_shape=(
            jax.ShapeDtypeStruct((32, BATCH, WIDTH), bf16),
            jax.ShapeDtypeStruct((2, 2, 8, 128), f32),
        ),
        in_specs=[pl.BlockSpec(memory_space=pl.ANY)] * 2,
        out_specs=[pl.BlockSpec(memory_space=pltpu.VMEM)] * 2,
        scratch_shapes=[
            pltpu.VMEM((SHARE, ROWS, WIDTH), bf16),
            pltpu.VMEM((WIDTH, COLUMNS), bf16),
            pltpu.VMEM((WIDTH, HEADS * HEAD_WIDTH), bf16),
            pltpu.VMEM((GROUPS, SHARE, ROWS, HEAD_WIDTH), bf16),
            pltpu.VMEM((2, SHARE, BACK[0] + ROWS, HEAD_WIDTH), bf16),
            pltpu.VMEM((2, SHARE, BACK[1] + ROWS, HEAD_WIDTH), bf16),
            pltpu.VMEM((2, SHARE, BACK[2] + ROWS, HEAD_WIDTH), bf16),
            pltpu.VMEM((BLOCK, KEYS), f32),
            pltpu.VMEM((SHARE, ROWS, HEAD_WIDTH), bf16),
            pltpu.VMEM((BATCH, 32, HEADS * HEAD_WIDTH), bf16),
            pltpu.VMEM((4, 8, 128), f32),
            pltpu.SemaphoreType.DMA((2,)),
            pltpu.SemaphoreType.DMA((TRANSFERS,)),
            pltpu.SemaphoreType.DMA((TRANSFERS,)),
        ],
        compiler_params=pltpu.CompilerParams(
            collective_id=0, has_side_effects=True, vmem_limit_bytes=60 * 1024 * 1024
        ),
    )(normed, piece)
    logs = logs[:, :, :SHARE, :].reshape(2, BATCH, 128)
    return (mixed, jnp.transpose(logs, (2, 1, 0)))


def solution(mesh):
    in_specs = (
        P(("sp", "tp"), None, None),
        P(),
        P(None, "sp", "tp"),
        P(None, "sp", "tp"),
        P(None, "sp", "tp"),
        P("tp", "sp"),
    )
    out_specs = (P(("sp", "tp"), None, None), P("sp", None, "tp"))
    return jax.shard_map(shards, mesh=mesh, in_specs=in_specs, out_specs=out_specs, check_vma=False)
```

```python
import functools
import math

import jax
import jax.numpy as jnp
from jax import lax
from jax.experimental import pallas as pl
from jax.experimental.pallas import tpu as pltpu
from jax.sharding import PartitionSpec as P

GROUPS = 3
HEADS = 8
HEAD_WIDTH = 128
STEPS = 24
DILATION_MIDDLE = 4
DILATION_WIDE = 16
WIDTH = 2048
BATCH = 6
SHARE = BATCH // 2
ROWS = 512
BACK = (128, 128, 384)
USED = (32, 96, 384)
WINDOW = (256, 256, 512)
KEYS = sum(WINDOW)
BLOCK = 128
PIECE = 64
COLUMNS = 10 * HEAD_WIDTH
ABSENT = -1e30

epsilon = 1e-06
MESH = pl.DeviceIdType.MESH


def rms_normed(widened, gain):
    scaled = widened * lax.rsqrt(jnp.mean(widened * widened, axis=-1, keepdims=True) + epsilon)
    return (scaled * gain).astype(jnp.bfloat16)


def dot(a, b):
    return lax.dot_general(a, b, (((1,), (0,)), ((), ())), preferred_element_type=jnp.float32)


def dot_t(a, b):
    return lax.dot_general(a, b, (((1,), (1,)), ((), ())), preferred_element_type=jnp.float32)


def kernel(
    tokens, gain, w_query, w_key, w_value, w_out, out, logs,
    gift, gift_out, toks, weights, whole_out, queries, near, middle, wide, bias,
    combined, arrived, log_rows, both_logs, own_sem, send_sem, recv_sem,
):
    s, x = lax.axis_index("sp"), lax.axis_index("tp")
    core, chip = lax.rem(s, 2), lax.div(s, 2)
    y, z = lax.rem(chip, 4), lax.div(chip, 4)

    def turn(value, by):
        return lax.rem(value + (by + 4), 4)

    def spot(y_at, z_at, core_at):
        return (z_at * 4 + y_at) * 2 + core_at

    zp, zm, xp, xm = (turn(v, d) for v in (z, x) for d in (1, -1))
    line = lax.rem(y, 2)
    pair_y, apart_y = y + 1 - 2 * line, turn(y, 2 * line - 1)
    share = lax.rem(lax.div(y + 1, 2), 2)
    other = 1 - core
    partner = (spot(y, z, other), x)
    z_plus, z_minus = (spot(y, zp, core), x), (spot(y, zm, core), x)
    x_plus, x_minus = (s, xp), (s, xm)
    upper = lax.div(y, 2)
    later = (spot(3 - y, turn(z, upper), core), x)
    corner = (spot(3 - y, turn(z, 2 * upper - 1), core), x)
    head = 2 * x + core

    crowd = []
    for flip_line in (0, 1):
        for flip_core in (0, 1):
            for step in range(4):
                if flip_line or flip_core or step:
                    y_at = pair_y if flip_line else y
                    core_at = other if flip_core else core
                    crowd.append((flip_line, flip_core, step, (spot(y_at, z, core_at), turn(x, step))))
    y_pair, y_apart = (spot(pair_y, z, core), x), (spot(apart_y, z, core), x)
    greeted = [c[3] for c in crowd] + [y_apart, z_plus, z_minus, corner]

    barrier = pltpu.get_barrier_semaphore()
    for device in greeted:
        pl.semaphore_signal(barrier, inc=1, device_id=device, device_id_type=MESH)

    started = []

    class Transfer:
        def __init__(self):
            self.index = len(started)
            started.append(self)

        def cover(self, src, dst, device):
            self.copy = pltpu.make_async_remote_copy(
                src_ref=src, dst_ref=dst, send_sem=send_sem.at[self.index],
                recv_sem=recv_sem.at[self.index], device_id=device, device_id_type=MESH,
            )

        def begin(self, src, dst, device):
            self.cover(src, dst, device)
            self.copy.start()

        def arrive(self):
            self.done = True
            self.copy.wait_recv()

    def send(src, dst, device):
        transfer = Transfer()
        transfer.begin(src, dst, device)
        return transfer

    def weight_rows(s_at, first=0, count=PIECE):
        return weights.at[pl.ds(pl.multiple_of(s_at * PIECE + first, 16), count), :]

    def token_rows(line_at, core_at, x_at):
        at = line_at * 256 + core_at * 128 + x_at * 32
        return toks.at[:, pl.ds(pl.multiple_of(at, 32), 32), :]

    parts = [(w, group) for group in (2, 1, 0) for w in (w_key, w_value)]
    parts += [(w_query, group) for group in (2, 1, 0)]
    rows = pl.ds(pl.multiple_of(s * PIECE, PIECE), PIECE)

    def part_of(index, core_at):
        w, group = parts[index]
        lanes = pl.ds(pl.multiple_of(core_at * HEAD_WIDTH, HEAD_WIDTH), HEAD_WIDTH)
        return (
            w.at[group, :, lanes],
            weights.at[rows, index * HEAD_WIDTH : (index + 1) * HEAD_WIDTH],
        )

    for index in range(9):
        pltpu.make_async_copy(*part_of(index, core), own_sem.at[0]).start()

    def turned(core_at):
        return w_out[:, pl.ds(pl.multiple_of(core_at * HEAD_WIDTH, HEAD_WIDTH), HEAD_WIDTH)]

    weights[rows, 9 * HEAD_WIDTH :] = turned(core)
    gift_out[...] = turned(other)
    def normed(b):
        return rms_normed(tokens[b].astype(jnp.float32), gain[...])

    place = pl.ds(pl.multiple_of(line * 256 + core * 128 + x * 32, 32), 32)
    for i in range(SHARE):
        toks[i, place, :] = normed(share * SHARE + i)
    for i in range(SHARE):
        gift[i] = normed((1 - share) * SHARE + i)

    pl.semaphore_wait(barrier, len(greeted))

    swap = Transfer()
    for index in range(9):
        src, dst = part_of(index, other)
        swap.begin(src, dst, partner)
    swap.begin(gift_out, weights.at[rows, 9 * HEAD_WIDTH :], partner)
    swap.cover(weight_rows(s), weight_rows(s), partner)
    whole = weights.at[rows, : 9 * HEAD_WIDTH]
    pltpu.make_async_copy(whole, whole, own_sem.at[0]).wait()

    class Ring:
        def __init__(self, rows_of, first, second, cut):
            self.rows_of, self.first, self.second, self.cut = rows_of, first, second, cut
            rows = rows_of(0)
            self.to_second = send(rows, rows, second)
            self.to_first = send(rows, rows, first)

        def onward(self):
            self.from_first_arrive()
            self.from_second_arrive()

    class ZRing(Ring):
        def from_first_arrive(self):
            self.to_second.arrive()
            rows = self.rows_of(-1, self.cut, PIECE - self.cut)
            self.on_second = send(rows, rows, self.second)

        def from_second_arrive(self):
            self.to_first.arrive()
            rows = self.rows_of(1, 0, self.cut)
            self.on_first = send(rows, rows, self.first)

        def far(self):
            self.on_second.arrive()
            self.on_first.arrive()

    class YRing(ZRing):
        def from_first_arrive(self):
            self.to_first.arrive()
            rows = self.rows_of("pair", self.cut, PIECE - self.cut)
            self.on_second = send(rows, rows, self.second)

        def from_second_arrive(self):
            self.to_second.arrive()
            rows = self.rows_of("apart", 0, self.cut)
            self.on_first = send(rows, rows, self.first)

    ys = {0: y, "pair": pair_y, "apart": apart_y, "far": turn(y, 2)}

    def y_ring(dz, core_at):
        return YRing(
            lambda step, *cut: weight_rows(spot(ys[step], turn(z, dz), core_at), *cut),
            y_pair, y_apart, 16,
        )

    def z_ring(dy, core_at):
        return ZRing(
            lambda step, *cut: weight_rows(spot(ys[dy], turn(z, step), core_at), *cut),
            z_minus, z_plus, 32,
        )

    own_first = y_ring(0, core)
    give = send(gift, toks.at[:, place, :], y_pair)
    own_second = {0: z_ring(0, core)}
    first = token_rows(line, core, x)
    tok_up = [send(first, first, x_plus)]
    tok_down = [send(first, first, x_minus)]
    tok_swap = [send(first, first, partner)]
    swap.arrive()
    their_first = z_ring(0, other)
    their_second = {0: y_ring(0, other)}

    near[:, :, : BACK[0] - USED[0], :] = jnp.zeros((2, SHARE, BACK[0] - USED[0], HEAD_WIDTH), jnp.bfloat16)
    middle[:, :, : BACK[1] - USED[1], :] = jnp.zeros((2, SHARE, BACK[1] - USED[1], HEAD_WIDTH), jnp.bfloat16)
    log_rows[...] = jnp.zeros_like(log_rows)
    left = 0
    for back, window, dilation in zip(BACK, WINDOW, (1, DILATION_MIDDLE, DILATION_WIDE)):
        query_at = lax.broadcasted_iota(jnp.int32, (BLOCK, window), 0)
        key_at = lax.broadcasted_iota(jnp.int32, (BLOCK, window), 1)
        lag = query_at + back - key_at
        allowed = (lag >= 0) & (lag <= STEPS * dilation) & ((lag & (dilation - 1)) == 0)
        bias[:, left : left + window] = jnp.where(allowed, jnp.float32(0), jnp.float32(ABSENT))
        left += window

    own_first.onward()
    own_second["pair"] = z_ring("pair", core)
    own_second["apart"] = z_ring("apart", core)
    own_second[0].onward()
    their_first.onward()
    their_second[-1] = y_ring(-1, other)
    their_second[1] = y_ring(1, other)
    their_second[0].onward()

    give.arrive()
    second = token_rows(1 - line, core, x)
    tok_up.append(send(second, second, x_plus))
    tok_down.append(send(second, second, x_minus))
    tok_swap.append(send(second, second, partner))
    tok_up[0].arrive()
    rows = token_rows(line, core, xm)
    tok_far_up = send(rows, rows, x_plus)
    tok_swap.append(send(rows, rows, partner))
    tok_down[0].arrive()
    rows = token_rows(line, core, xp)
    tok_swap.append(send(rows, rows, partner))

    own_first.far()
    own_second["far"] = z_ring("far", core)
    their_first.far()
    their_second[2] = y_ring(2, other)
    for y_step, z_step in (("pair", -1), ("apart", 1)):
        own_second[y_step].onward()
        their_second[z_step].onward()

    tok_down[1].arrive()
    rows = token_rows(1 - line, core, xp)
    tok_far_down = send(rows, rows, x_minus)
    tok_swap.append(send(rows, rows, partner))
    tok_up[1].arrive()
    rows = token_rows(1 - line, core, xm)
    tok_swap.append(send(rows, rows, partner))

    own_second["far"].onward()
    their_second[2].onward()
    for y_step, z_step in zip(ys, (0, -1, 1, 2)):
        own_second[y_step].far()
        their_second[z_step].far()
    tok_far_up.arrive()
    rows = token_rows(line, core, turn(x, 2))
    tok_swap.append(send(rows, rows, partner))
    tok_far_down.arrive()
    rows = token_rows(1 - line, core, turn(x, 2))
    tok_swap.append(send(rows, rows, partner))

    def head_columns(x_at, core_at, half=None):
        lanes = pl.ds(pl.multiple_of((2 * x_at + core_at) * HEAD_WIDTH, HEAD_WIDTH), HEAD_WIDTH)
        if half is None:
            return whole_out.at[:, lanes]
        return whole_out.at[pl.ds(half * (WIDTH // 2), WIDTH // 2), lanes]

    out_rows = weights.at[:, 9 * HEAD_WIDTH :]
    mine_o = head_columns(x, core)
    out_up = send(out_rows, mine_o, x_plus)
    out_down = send(out_rows, mine_o, x_minus)
    out_swap = [send(out_rows, mine_o, partner)]
    whole_out[:, pl.ds(pl.multiple_of(head * HEAD_WIDTH, HEAD_WIDTH), HEAD_WIDTH)] = weights[:, 9 * HEAD_WIDTH :]

    for copy in tok_swap:
        copy.arrive()

    def project(left, width, b):
        return dot(toks[b], weights[:, left : left + width]).astype(jnp.bfloat16)

    groups = ((wide, 2), (middle, 1), (near, 0))
    halo = []
    for b in range(SHARE):
        sent = []
        for at, (keys, group) in enumerate(groups):
            back, used = BACK[group], USED[group]
            both = project(at * 2 * HEAD_WIDTH, 2 * HEAD_WIDTH, b)
            keys[0, b, back:, :] = both[:, :HEAD_WIDTH]
            keys[1, b, back:, :] = both[:, HEAD_WIDTH:]
            sent.append(
                send(
                    keys.at[:, b, back + ROWS - used :, :],
                    keys.at[:, b, back - used : back, :],
                    later,
                )
            )
        halo.append(sent)

    def ask(b):
        both = project(6 * HEAD_WIDTH, 2 * HEAD_WIDTH, b)
        queries[2, b] = both[:, :HEAD_WIDTH]
        queries[1, b] = both[:, HEAD_WIDTH:]
        queries[0, b] = project(8 * HEAD_WIDTH, HEAD_WIDTH, b)

    ask(0)
    out_up.arrive()
    rows = head_columns(xm, core, 0)
    out_far_up = send(rows, rows, x_plus)
    rows = head_columns(xm, core)
    out_swap.append(send(rows, rows, partner))
    out_down.arrive()
    rows = head_columns(xp, core, 1)
    out_far_down = send(rows, rows, x_minus)
    rows = head_columns(xp, core)
    out_swap.append(send(rows, rows, partner))
    ask(1)
    ask(2)

    factor = math.log2(math.e) / math.sqrt(HEAD_WIDTH)
    start_at = (z * 2 + upper) * ROWS
    lanes = pl.ds(pl.multiple_of(head * HEAD_WIDTH, HEAD_WIDTH), HEAD_WIDTH)

    def rows_for(line_at, core_at, x_at):
        return pl.ds(pl.multiple_of(line_at * 256 + core_at * 128 + x_at * 32, 32), 32)

    exchange = []
    for b in range(SHARE):
        for copy in halo[b]:
            copy.arrive()

        def attend(block, carry, b=b):
            at = pl.multiple_of(block * BLOCK, BLOCK)
            scores, left = [], 0
            for group, keys in enumerate((near, middle, wide)):
                window = WINDOW[group]
                score = dot_t(queries[group, b, pl.ds(at, BLOCK), :], keys[0, b, pl.ds(at, window), :])
                key_at = lax.broadcasted_iota(jnp.int32, (1, window), 1) + (start_at + at - BACK[group])
                edge = jnp.where(key_at >= 0, jnp.float32(0), jnp.float32(ABSENT))
                scores.append(score * factor + (bias[:, left : left + window] + edge))
                left += window
            peak = functools.reduce(
                jnp.maximum, [jnp.max(score, axis=1, keepdims=True) for score in scores]
            )
            total, mixed = 0.0, 0.0
            for group, keys in enumerate((near, middle, wide)):
                lifted = jnp.exp2(scores[group] - peak)
                total = total + jnp.sum(lifted, axis=1, keepdims=True)
                mixed = mixed + dot(
                    lifted.astype(jnp.bfloat16), keys[1, b, pl.ds(at, WINDOW[group]), :]
                )
            combined[b, pl.ds(at, BLOCK), :] = (mixed / total).astype(jnp.bfloat16)
            log = (peak + jnp.log2(total)) * math.log(2.0)
            log_rows[block, b : b + 1, :] = jnp.transpose(
                jnp.broadcast_to(log, (BLOCK, BLOCK))
            )[0:1, :]
            return carry

        lax.fori_loop(0, 4, attend, 0)

        for flip_line, flip_core, step, device in crowd:
            line_at = 1 - line if flip_line else line
            core_at = other if flip_core else core
            exchange.append(
                send(
                    combined.at[b, rows_for(line_at, core_at, turn(x, step)), :],
                    arrived.at[share * SHARE + b, :, lanes],
                    device,
                )
            )
            if step == 0 and b == SHARE - 1:
                exchange.append(send(log_rows.at[line_at * 2 + core_at], both_logs.at[core, share], device))
        arrived[share * SHARE + b, :, lanes] = combined[b, rows_for(line, core, x), :]
        if b == 0:
            out_far_up.arrive()
            rows = head_columns(turn(x, 2), core, 0)
            out_swap.append(send(rows, rows, partner))
            out_far_down.arrive()
            rows = head_columns(turn(x, 2), core, 1)
            out_swap.append(send(rows, rows, partner))
    both_logs[core, share] = log_rows[line * 2 + core]
    for copy in out_swap + exchange:
        copy.arrive()

    everything = arrived[...].reshape(192, HEADS * HEAD_WIDTH)
    for tile in range(8):
        part = dot_t(everything, whole_out[tile * 256 : (tile + 1) * 256, :]).astype(jnp.bfloat16)
        out[:, :, tile * 256 : (tile + 1) * 256] = part.reshape(BATCH, 32, 256)
    for core_at in range(2):
        for share_at in range(2):
            for b in range(SHARE):
                logs[share_at * SHARE + b, core_at : core_at + 1, :] = both_logs[core_at, share_at, b : b + 1, :]

    for transfer in started:
        transfer.copy.wait_send()


TRANSFERS = 130


def shards(tokens, norm_gain, w_query, w_key, w_value, w_out):
    bf16, f32 = jnp.bfloat16, jnp.float32
    mixed, logs = pl.pallas_call(
        kernel,
        out_shape=(
            jax.ShapeDtypeStruct((BATCH, 32, WIDTH), bf16),
            jax.ShapeDtypeStruct((BATCH, 2, 128), f32),
        ),
        in_specs=[pl.BlockSpec(memory_space=pltpu.VMEM)] * 2
        + [pl.BlockSpec(memory_space=pl.ANY)] * 3
        + [pl.BlockSpec(memory_space=pltpu.VMEM)],
        out_specs=[pl.BlockSpec(memory_space=pltpu.VMEM)] * 2,
        scratch_shapes=[
            pltpu.VMEM((SHARE, 32, WIDTH), bf16),
            pltpu.VMEM((PIECE, HEAD_WIDTH), bf16),
            pltpu.VMEM((SHARE, ROWS, WIDTH), bf16),
            pltpu.VMEM((WIDTH, COLUMNS), bf16),
            pltpu.VMEM((WIDTH, HEADS * HEAD_WIDTH), bf16),
            pltpu.VMEM((GROUPS, SHARE, ROWS, HEAD_WIDTH), bf16),
            pltpu.VMEM((2, SHARE, BACK[0] + ROWS, HEAD_WIDTH), bf16),
            pltpu.VMEM((2, SHARE, BACK[1] + ROWS, HEAD_WIDTH), bf16),
            pltpu.VMEM((2, SHARE, BACK[2] + ROWS, HEAD_WIDTH), bf16),
            pltpu.VMEM((BLOCK, KEYS), f32),
            pltpu.VMEM((SHARE, ROWS, HEAD_WIDTH), bf16),
            pltpu.VMEM((BATCH, 32, HEADS * HEAD_WIDTH), bf16),
            pltpu.VMEM((4, 8, 128), f32),
            pltpu.VMEM((2, 2, 8, 128), f32),
            pltpu.SemaphoreType.DMA((1,)),
            pltpu.SemaphoreType.DMA((TRANSFERS,)),
            pltpu.SemaphoreType.DMA((TRANSFERS,)),
        ],
        compiler_params=pltpu.CompilerParams(
            collective_id=0, has_side_effects=True, vmem_limit_bytes=44 * 1024 * 1024
        ),
    )(
        jnp.transpose(tokens, (1, 0, 2)), norm_gain.reshape(1, WIDTH),
        w_query, w_key, w_value, jnp.transpose(w_out),
    )
    return (jnp.transpose(mixed, (1, 0, 2)), jnp.transpose(logs, (2, 0, 1)))


def solution(mesh):
    in_specs = (
        P(("sp", "tp"), None, None),
        P(),
        P(None, "sp", "tp"),
        P(None, "sp", "tp"),
        P(None, "sp", "tp"),
        P("tp", "sp"),
    )
    out_specs = (P(("sp", "tp"), None, None), P("sp", None, "tp"))
    return jax.shard_map(shards, mesh=mesh, in_specs=in_specs, out_specs=out_specs, check_vma=False)
```

```python
import functools
import math

import jax
import jax.numpy as jnp
from jax import lax
from jax.experimental import pallas as pl
from jax.experimental.pallas import tpu as pltpu
from jax.sharding import PartitionSpec as P

GROUPS = 3
HEADS = 8
HEAD_WIDTH = 128
STEPS = 24
DILATION_MIDDLE = 4
DILATION_WIDE = 16
WIDTH = 2048
BATCH = 6
SHARE = BATCH // 2
ROWS = 512
AHEAD = (1, 1, 3)
BLOCK = 128
BLOCKS = ROWS // BLOCK
WINDOW = tuple((ahead + 1) * BLOCK for ahead in AHEAD)
KEYS = sum(WINDOW)
PIECE = 64
COLUMNS = 10 * HEAD_WIDTH
UNITS = ((0, 5 * HEAD_WIDTH), (5 * HEAD_WIDTH, 10 * HEAD_WIDTH))
ABSENT = -1e30

epsilon = 1e-06
MESH = pl.DeviceIdType.MESH


def rms_normed(widened, gain):
    scaled = widened * lax.rsqrt(jnp.mean(widened * widened, axis=-1, keepdims=True) + epsilon)
    return (scaled * gain).astype(jnp.bfloat16)


def dot(a, b):
    return lax.dot_general(a, b, (((1,), (0,)), ((), ())), preferred_element_type=jnp.float32)


def dot_t(a, b):
    return lax.dot_general(a, b, (((1,), (1,)), ((), ())), preferred_element_type=jnp.float32)


def kernel(
    tokens, gain, w_query, w_key, w_value, w_out, out, logs,
    raw, gains, gift, toks, weights, whole_out, queries, near, middle, wide, bias,
    combined, arrived, log_rows, both_logs, own_sem, send_sem, recv_sem,
):
    s, x = lax.axis_index("sp"), lax.axis_index("tp")
    core, chip = lax.rem(s, 2), lax.div(s, 2)
    y, z = lax.rem(chip, 4), lax.div(chip, 4)

    def turn(value, by):
        return lax.rem(value + (by + 4), 4)

    def spot(y_at, z_at, core_at):
        return (z_at * 4 + y_at) * 2 + core_at

    zp, zm, xp, xm = (turn(v, d) for v in (z, x) for d in (1, -1))
    line = lax.rem(y, 2)
    pair_y, apart_y = y + 1 - 2 * line, turn(y, 2 * line - 1)
    share = lax.rem(lax.div(y + 1, 2), 2)
    other = 1 - core
    partner = (spot(y, z, other), x)
    z_plus, z_minus = (spot(y, zp, core), x), (spot(y, zm, core), x)
    x_plus, x_minus = (s, xp), (s, xm)
    upper = lax.div(y, 2)
    later = (spot(3 - y, turn(z, upper), core), x)
    head = 2 * x + core

    crowd = []
    for flip_line in (0, 1):
        for flip_core in (0, 1):
            for step in range(4):
                if flip_line or flip_core or step:
                    y_at = pair_y if flip_line else y
                    core_at = other if flip_core else core
                    crowd.append((flip_line, flip_core, step, (spot(y_at, z, core_at), turn(x, step))))
    y_pair, y_apart = (spot(pair_y, z, core), x), (spot(apart_y, z, core), x)
    greeted = [partner, x_plus, x_minus, y_pair, y_apart, z_plus, z_minus]

    barrier = pltpu.get_barrier_semaphore()
    for device in greeted:
        pl.semaphore_signal(barrier, inc=1, device_id=device, device_id_type=MESH)

    counts, opened = [0], [0]

    def tiles_of(ref):
        return math.prod(ref.shape) * ref.dtype.itemsize // 4096

    def shape_of(count):
        for across_at in range(10, 0, -1):
            if count % across_at == 0 and count // across_at <= WIDTH // 16:
                return count // across_at, across_at
        return None

    def extent(count):
        down, over = shape_of(count)
        return weights.at[: down * 16, : over * HEAD_WIDTH]

    class Transfer:
        def __init__(self):
            self.index = opened[0]
            opened[0] += 1
            self.count = 0

        def begin(self, src, dst, device):
            count = tiles_of(src)
            if counts[-1] >= 560 and shape_of(counts[-1]):
                counts.append(0)
            counts[-1] += count
            self.count += count
            pltpu.make_async_remote_copy(
                src_ref=src, dst_ref=dst, send_sem=send_sem.at[len(counts) - 1],
                recv_sem=recv_sem.at[self.index], device_id=device, device_id_type=MESH,
            ).start()

        def arrive(self):
            self.done = True
            whole = extent(self.count)
            pltpu.make_async_copy(whole, whole, recv_sem.at[self.index]).wait()

    def send(src, dst, device):
        transfer = Transfer()
        transfer.begin(src, dst, device)
        return transfer

    def weight_rows(s_at, unit, first=0, count=PIECE):
        left, right = UNITS[unit]
        return weights.at[pl.ds(pl.multiple_of(s_at * PIECE + first, 16), count), left:right]

    def token_rows(line_at, core_at, x_at, b):
        return toks.at[x_at, b, line_at * 2 + core_at]

    take_tokens = pltpu.make_async_copy(tokens, raw, own_sem.at[0])
    take_gain = pltpu.make_async_copy(gain, gains, own_sem.at[1])
    take_tokens.start()
    take_gain.start()
    parts = [(w, group) for group in (2, 1) for w in (w_key, w_value)] + [(w_out, None)]
    parts += [(w_key, 0), (w_value, 0)] + [(w_query, group) for group in (2, 1, 0)]
    rows = pl.ds(pl.multiple_of(s * PIECE, PIECE), PIECE)

    def part_of(index, core_at):
        w, group = parts[index]
        lanes = pl.ds(pl.multiple_of(core_at * HEAD_WIDTH, HEAD_WIDTH), HEAD_WIDTH)
        src = w.at[:, lanes] if group is None else w.at[group, :, lanes]
        return src, weights.at[rows, index * HEAD_WIDTH : (index + 1) * HEAD_WIDTH]

    for index in range(10):
        pltpu.make_async_copy(*part_of(index, core), own_sem.at[2 + index // 5]).start()

    def normed(b):
        return rms_normed(raw[b].astype(jnp.float32), gains[...])

    take_tokens.wait()
    take_gain.wait()
    for b in range(SHARE):
        toks[x, b, line * 2 + core] = normed(share * SHARE + b)
    for b in range(SHARE):
        gift[b] = normed((1 - share) * SHARE + b)

    pl.semaphore_wait(barrier, len(greeted))

    swap = []
    for unit in (0, 1):
        swap.append(Transfer())
        for index in range(5 * unit, 5 * unit + 5):
            src, dst = part_of(index, other)
            swap[unit].begin(src, dst, partner)

    class Ring:
        def __init__(self, rows_of, first, second, cut):
            self.rows_of, self.first, self.second, self.cut = rows_of, first, second, cut
            rows = rows_of(0)
            self.to_second = send(rows, rows, second)
            self.to_first = send(rows, rows, first)

        def onward(self):
            self.from_first_arrive()
            self.from_second_arrive()

    class ZRing(Ring):
        def from_first_arrive(self):
            self.to_second.arrive()
            rows = self.rows_of(-1, self.cut, PIECE - self.cut)
            self.on_second = send(rows, rows, self.second)

        def from_second_arrive(self):
            self.to_first.arrive()
            rows = self.rows_of(1, 0, self.cut)
            self.on_first = send(rows, rows, self.first)

        def far(self):
            self.on_second.arrive()
            self.on_first.arrive()

    class YRing(ZRing):
        def from_first_arrive(self):
            self.to_first.arrive()
            rows = self.rows_of("pair", self.cut, PIECE - self.cut)
            self.on_second = send(rows, rows, self.second)

        def from_second_arrive(self):
            self.to_second.arrive()
            rows = self.rows_of("apart", 0, self.cut)
            self.on_first = send(rows, rows, self.first)

    ys = {0: y, "pair": pair_y, "apart": apart_y, "far": turn(y, 2)}

    def y_ring(dz, core_at, unit):
        return YRing(
            lambda step, *cut: weight_rows(spot(ys[step], turn(z, dz), core_at), unit, *cut),
            y_pair, y_apart, 48,
        )

    def z_ring(dy, core_at, unit):
        return ZRing(
            lambda step, *cut: weight_rows(spot(ys[dy], turn(z, step), core_at), unit, *cut),
            z_minus, z_plus, 48,
        )

    across = {step: Transfer() for step in (0, -1, 1, 2)}
    give = [None] * SHARE

    def token_steps():
        up, down, far_up, far_down = {}, {}, {}, {}

        def cross(step, line_at, b):
            rows = token_rows(line_at, core, turn(x, step), b)
            across[step].begin(rows, rows, partner)

        def launch(line_at, b):
            rows = token_rows(line_at, core, x, b)
            which = 0 if line_at is line else 1
            up[which, b] = send(rows, rows, x_plus)
            down[which, b] = send(rows, rows, x_minus)
            cross(0, line_at, b)

        def onward(which, step, b):
            line_at = (line, far_line)[which]
            (up if step == -1 else down)[which, b].arrive()
            if (which, step) in ((0, -1), (1, 1)):
                rows = token_rows(line_at, core, turn(x, step), b)
                if step == -1:
                    far_up[b] = send(rows, rows, x_plus)
                else:
                    far_down[b] = send(rows, rows, x_minus)
            cross(step, line_at, b)

        far_line = 1 - line
        for b in range(SHARE):
            launch(line, b)
        yield
        for b in range(SHARE):
            give[b].arrive()
            launch(far_line, b)
            yield
        for b in range(SHARE):
            onward(0, -1, b)
            onward(0, 1, b)
            yield
        for b in range(SHARE):
            onward(1, 1, b)
            onward(1, -1, b)
            yield
        for b in range(SHARE):
            far_up[b].arrive()
            cross(2, line, b)
            far_down[b].arrive()
            cross(2, far_line, b)
            yield

    def weight_steps(unit):
        own, their = {}, {}
        whole = weight_rows(s, unit)
        pltpu.make_async_copy(whole, whole, own_sem.at[2 + unit]).wait()
        own["first"] = y_ring(0, core, unit)
        own[0] = z_ring(0, core, unit)
        yield
        swap[unit].arrive()
        their["first"] = z_ring(0, other, unit)
        their[0] = y_ring(0, other, unit)
        yield
        own["first"].onward()
        own["pair"] = z_ring("pair", core, unit)
        own["apart"] = z_ring("apart", core, unit)
        own[0].onward()
        yield
        their["first"].onward()
        their[-1] = y_ring(-1, other, unit)
        their[1] = y_ring(1, other, unit)
        their[0].onward()
        yield
        own["first"].far()
        own["far"] = z_ring("far", core, unit)
        their["first"].far()
        their[2] = y_ring(2, other, unit)
        yield
        for y_step, z_step in (("pair", -1), ("apart", 1)):
            own[y_step].onward()
            their[z_step].onward()
            yield
        own["far"].onward()
        their[2].onward()
        yield
        for y_step, z_step in zip(ys, (0, -1, 1, 2)):
            own[y_step].far()
            their[z_step].far()
        yield

    steps = {"t": token_steps(), "0": weight_steps(0), "1": weight_steps(1)}

    def go(order):
        for which in order.replace(" ", ""):
            next(steps[which])

    give[0] = send(gift.at[0], token_rows(line, core, x, 0), y_pair)
    go("0t")
    give[1] = send(gift.at[1], token_rows(line, core, x, 1), y_pair)
    go("01")
    give[2] = send(gift.at[2], token_rows(line, core, x, 2), y_pair)

    near[:, :, 0, :96, :] = jnp.zeros((2, SHARE, 96, HEAD_WIDTH), jnp.bfloat16)
    log_rows[...] = jnp.zeros_like(log_rows)
    left = 0
    for ahead, window, dilation in zip(AHEAD, WINDOW, (1, DILATION_MIDDLE, DILATION_WIDE)):
        query_at = lax.broadcasted_iota(jnp.int32, (BLOCK, window), 0)
        key_at = lax.broadcasted_iota(jnp.int32, (BLOCK, window), 1)
        lag = query_at + ahead * BLOCK - key_at
        allowed = (lag >= 0) & (lag <= STEPS * dilation) & ((lag & (dilation - 1)) == 0)
        bias[:, left : left + window] = jnp.where(allowed, jnp.float32(0), jnp.float32(ABSENT))
        left += window

    def project(x_at, left, width):
        rows = toks[x_at].reshape(SHARE * BLOCKS * 32, WIDTH)
        return dot(rows, weights[:, left : left + width]).astype(jnp.bfloat16)

    def block_rows(x_at):
        return pl.ds(pl.multiple_of(x_at * 32, 32), 32)

    def lay(found, left, buffer, x_at, ahead):
        part = found[:, left : left + HEAD_WIDTH].reshape(SHARE, BLOCKS, 32, HEAD_WIDTH)
        buffer[:, ahead : ahead + BLOCKS, block_rows(x_at), :] = part

    def keys_of(step):
        x_at = turn(x, step)
        across[step].arrive()
        for place, (keys, group) in enumerate(((wide, 2), (middle, 1))):
            found = project(x_at, place * 2 * HEAD_WIDTH, 2 * HEAD_WIDTH)
            for which in (0, 1):
                lay(found, which * HEAD_WIDTH, keys.at[which], x_at, AHEAD[group])

    halo = []

    def pass_on(keys, group, x_at, share_at):
        ahead = AHEAD[group]
        halo.append(
            send(
                keys.at[:, share_at, BLOCKS:, block_rows(x_at), :],
                keys.at[:, share_at, :ahead, block_rows(x_at), :],
                later,
            )
        )

    def pass_all(step):
        for keys, group in ((wide, 2), (middle, 1)):
            pass_on(keys, group, turn(x, step), slice(None))

    def head_columns(x_at, core_at, half=None):
        lanes = pl.ds(pl.multiple_of((2 * x_at + core_at) * HEAD_WIDTH, HEAD_WIDTH), HEAD_WIDTH)
        if half is None:
            return whole_out.at[:, lanes]
        return whole_out.at[pl.ds(half * (WIDTH // 2), WIDTH // 2), lanes]

    out_swap = []

    def out_steps():
        out_rows = weights.at[:, 4 * HEAD_WIDTH : 5 * HEAD_WIDTH]
        mine = head_columns(x, core)
        up = send(out_rows, mine, x_plus)
        down = send(out_rows, mine, x_minus)
        out_swap.append(send(out_rows, mine, partner))
        lanes = pl.ds(pl.multiple_of(head * HEAD_WIDTH, HEAD_WIDTH), HEAD_WIDTH)
        whole_out[:, lanes] = weights[:, 4 * HEAD_WIDTH : 5 * HEAD_WIDTH]
        yield
        up.arrive()
        rows = head_columns(xm, core, 0)
        far_up = send(rows, rows, x_plus)
        rows = head_columns(xm, core)
        out_swap.append(send(rows, rows, partner))
        down.arrive()
        rows = head_columns(xp, core, 1)
        far_down = send(rows, rows, x_minus)
        rows = head_columns(xp, core)
        out_swap.append(send(rows, rows, partner))
        yield
        far_up.arrive()
        rows = head_columns(turn(x, 2), core, 0)
        out_swap.append(send(rows, rows, partner))
        far_down.arrive()
        rows = head_columns(turn(x, 2), core, 1)
        out_swap.append(send(rows, rows, partner))
        yield

    steps["o"] = out_steps()

    go("00t1t0t1t0t10t100tt")
    keys_of(0)
    pass_all(0)
    go("1to11")
    keys_of(-1)
    pass_all(-1)
    keys_of(1)
    pass_all(1)
    go("ttt")
    keys_of(2)
    for b in range(SHARE):
        for keys, group in ((wide, 2), (middle, 1)):
            pass_on(keys, group, turn(x, 2), pl.ds(b, 1))
    go("1")

    def keys_near(x_at, carry):
        found = project(x_at, UNITS[1][0], 2 * HEAD_WIDTH)
        for which in (0, 1):
            lay(found, which * HEAD_WIDTH, near.at[which], x_at, AHEAD[0])
        return carry

    lax.fori_loop(0, 4, keys_near, 0)
    near_halo = send(near.at[:, :, BLOCKS, 96:, :], near.at[:, :, 0, 96:, :], later)

    def ask(x_at, carry):
        left = UNITS[1][0] + 2 * HEAD_WIDTH
        found = project(x_at, left, 2 * HEAD_WIDTH)
        lay(found, 0, queries.at[2], x_at, 0)
        lay(found, HEAD_WIDTH, queries.at[1], x_at, 0)
        lay(project(x_at, left + 2 * HEAD_WIDTH, HEAD_WIDTH), 0, queries.at[0], x_at, 0)
        return carry

    lax.fori_loop(0, 4, ask, 0)

    factor = math.log2(math.e) / math.sqrt(HEAD_WIDTH)
    start_at = (z * 2 + upper) * ROWS
    lanes = pl.ds(pl.multiple_of(head * HEAD_WIDTH, HEAD_WIDTH), HEAD_WIDTH)

    def attend(b, block):
        scores, left = [], 0
        for group, keys in enumerate((near, middle, wide)):
            window = WINDOW[group]
            seen = keys[0, b, block : block + AHEAD[group] + 1].reshape(window, HEAD_WIDTH)
            score = dot_t(queries[group, b, block], seen)
            first = start_at + (block - AHEAD[group]) * BLOCK
            hidden = bias[:, left : left + window]
            if block < AHEAD[group]:
                key_at = lax.broadcasted_iota(jnp.int32, (1, window), 1) + first
                hidden = hidden + jnp.where(key_at >= 0, jnp.float32(0), jnp.float32(ABSENT))
            scores.append(score * factor + hidden)
            left += window
        peak = functools.reduce(
            jnp.maximum, [jnp.max(score, axis=1, keepdims=True) for score in scores]
        )
        total, mixed = 0.0, 0.0
        for group, keys in enumerate((near, middle, wide)):
            lifted = jnp.exp2(scores[group] - peak)
            total = total + jnp.sum(lifted, axis=1, keepdims=True)
            seen = keys[1, b, block : block + AHEAD[group] + 1].reshape(WINDOW[group], HEAD_WIDTH)
            mixed = mixed + dot(lifted.astype(jnp.bfloat16), seen)
        combined[b, block * BLOCK : (block + 1) * BLOCK, :] = (mixed / total).astype(jnp.bfloat16)
        log = (peak + jnp.log2(total)) * math.log(2.0)
        log_rows[block, b : b + 1, :] = jnp.transpose(jnp.broadcast_to(log, (BLOCK, BLOCK)))[0:1, :]

    def rows_for(line_at, core_at, x_at):
        return pl.ds(pl.multiple_of(line_at * 256 + core_at * 128 + x_at * 32, 32), 32)

    for b in range(SHARE):
        attend(b, BLOCKS - 1)
    go("o")
    near_halo.arrive()
    for copy in halo[:6]:
        copy.arrive()
    exchange = Transfer()
    for b in range(SHARE):
        halo[6 + 2 * b].arrive()
        halo[7 + 2 * b].arrive()
        for block in range(BLOCKS - 1):
            attend(b, block)

        for flip_line, flip_core, step, device in crowd:
            line_at = 1 - line if flip_line else line
            core_at = other if flip_core else core
            exchange.begin(
                combined.at[b, rows_for(line_at, core_at, turn(x, step)), :],
                arrived.at[share * SHARE + b, :, lanes],
                device,
            )
            if step == 0 and b == SHARE - 1:
                exchange.begin(
                    log_rows.at[line_at * 2 + core_at], both_logs.at[core, share], device
                )
        arrived[share * SHARE + b, :, lanes] = combined[b, rows_for(line, core, x), :]
        if b == 0:
            go("o")
    both_logs[core, share] = log_rows[line * 2 + core]
    for copy in out_swap + [exchange]:
        copy.arrive()

    everything = arrived[...].reshape(192, HEADS * HEAD_WIDTH)
    for tile in range(8):
        part = dot_t(everything, whole_out[tile * 256 : (tile + 1) * 256, :]).astype(jnp.bfloat16)
        out[:, :, tile * 256 : (tile + 1) * 256] = part.reshape(BATCH, 32, 256)
    for core_at in range(2):
        for share_at in range(2):
            for b in range(SHARE):
                logs[share_at * SHARE + b, core_at : core_at + 1, :] = both_logs[core_at, share_at, b : b + 1, :]

    assert opened[0] <= ARRIVALS and len(counts) <= SENDS, (opened, counts)
    for index, count in enumerate(counts):
        whole = extent(count)
        pltpu.make_async_copy(whole, whole, send_sem.at[index]).wait()


ARRIVALS = 130
SENDS = 8


def shards(tokens, norm_gain, w_query, w_key, w_value, w_out):
    bf16, f32 = jnp.bfloat16, jnp.float32
    operands = (
        jnp.transpose(tokens, (1, 0, 2)), norm_gain.reshape(1, WIDTH),
        w_query, w_key, w_value, jnp.transpose(w_out),
    )
    mixed, logs = pl.pallas_call(
        kernel,
        out_shape=(
            jax.ShapeDtypeStruct((BATCH, 32, WIDTH), bf16),
            jax.ShapeDtypeStruct((BATCH, 2, 128), f32),
        ),
        in_specs=[pl.BlockSpec(memory_space=pltpu.HBM)] * 6,
        out_specs=[pl.BlockSpec(memory_space=pltpu.VMEM)] * 2,
        scratch_shapes=[
            pltpu.VMEM((BATCH, 32, WIDTH), bf16),
            pltpu.VMEM((1, WIDTH), f32),
            pltpu.VMEM((SHARE, 32, WIDTH), bf16),
            pltpu.VMEM((4, SHARE, BLOCKS, 32, WIDTH), bf16),
            pltpu.VMEM((WIDTH, COLUMNS), bf16),
            pltpu.VMEM((WIDTH, HEADS * HEAD_WIDTH), bf16),
            pltpu.VMEM((GROUPS, SHARE, BLOCKS, BLOCK, HEAD_WIDTH), bf16),
            pltpu.VMEM((2, SHARE, AHEAD[0] + BLOCKS, BLOCK, HEAD_WIDTH), bf16),
            pltpu.VMEM((2, SHARE, AHEAD[1] + BLOCKS, BLOCK, HEAD_WIDTH), bf16),
            pltpu.VMEM((2, SHARE, AHEAD[2] + BLOCKS, BLOCK, HEAD_WIDTH), bf16),
            pltpu.VMEM((BLOCK, KEYS), f32),
            pltpu.VMEM((SHARE, ROWS, HEAD_WIDTH), bf16),
            pltpu.VMEM((BATCH, 32, HEADS * HEAD_WIDTH), bf16),
            pltpu.VMEM((4, 8, 128), f32),
            pltpu.VMEM((2, 2, 8, 128), f32),
            pltpu.SemaphoreType.DMA((4,)),
            pltpu.SemaphoreType.DMA((SENDS,)),
            pltpu.SemaphoreType.DMA((ARRIVALS,)),
        ],
        compiler_params=pltpu.CompilerParams(
            collective_id=0, has_side_effects=True, vmem_limit_bytes=44 * 1024 * 1024
        ),
    )(*(pltpu.with_memory_space_constraint(array, pltpu.HBM) for array in operands))
    return (jnp.transpose(mixed, (1, 0, 2)), jnp.transpose(logs, (2, 0, 1)))


def solution(mesh):
    in_specs = (
        P(("sp", "tp"), None, None),
        P(),
        P(None, "sp", "tp"),
        P(None, "sp", "tp"),
        P(None, "sp", "tp"),
        P("tp", "sp"),
    )
    out_specs = (P(("sp", "tp"), None, None), P("sp", None, "tp"))
    return jax.shard_map(shards, mesh=mesh, in_specs=in_specs, out_specs=out_specs, check_vma=False)
```

```python
import functools
import math

import jax
import jax.numpy as jnp
from jax import lax
from jax.experimental import pallas as pl
from jax.experimental.pallas import tpu as pltpu
from jax.sharding import PartitionSpec as P

GROUPS = 3
HEADS = 8
HEAD_WIDTH = 128
STEPS = 24
DILATION_MIDDLE = 4
DILATION_WIDE = 16
WIDTH = 2048
BATCH = 6
SHARE = BATCH // 2
ROWS = 512
AHEAD = (1, 1, 3)
BLOCK = 128
BLOCKS = ROWS // BLOCK
WINDOW = tuple((ahead + 1) * BLOCK for ahead in AHEAD)
KEYS = sum(WINDOW)
PIECE = 64
COLUMNS = 10 * HEAD_WIDTH
UNITS = ((0, 5 * HEAD_WIDTH), (5 * HEAD_WIDTH, 10 * HEAD_WIDTH))
ABSENT = -1e30
ORDER = (
    "t00", "O0", "G0", "t01", "t02", "R0", "G1", "G2", "Op0", "Oa0", "Zm00", "Zp00", "up00",
    "dn00", "Rm0", "Rp0", "Ya00", "g0", "up01", "dn01", "Zmp0", "Zpp0", "Yp00", "Zma0",
    "Zpa0", "Yam0", "O1", "up02", "dn02", "g1", "Rf0", "Yap0", "dn10", "fu0", "R1", "Of0",
    "g2", "Zm01", "Zp01", "Oa1", "Ypm0", "up10", "dn11", "Yaf0", "Ypp0", "Rm1", "fu1", "Rp1",
    "fd0", "Zmf0", "Zpf0", "Op1", "Ya01", "Ypf0", "fu2", "dn12", "Zma1", "Zpa1", "Yp01",
    "Rf1", "Yam1", "up11", "fd1", "Of1", "Yap1", "Zmp1", "Zpp1", "Ypm1", "W0", "o0", "K0",
    "up12", "fd2", "Ypp1", "Yaf1", "Zmf1", "Zpf1", "Km", "Ypf1", "Kp", "K2", "W1", "N", "oum",
    "odm", "Q",
)
Y_CUT = (0, 64)
Z_CUT = (32, 32)

epsilon = 1e-06
MESH = pl.DeviceIdType.MESH


def rms_normed(widened, gain):
    scaled = widened * lax.rsqrt(jnp.mean(widened * widened, axis=-1, keepdims=True) + epsilon)
    return (scaled * gain).astype(jnp.bfloat16)


def dot(a, b):
    return lax.dot_general(a, b, (((1,), (0,)), ((), ())), preferred_element_type=jnp.float32)


def dot_t(a, b):
    return lax.dot_general(a, b, (((1,), (1,)), ((), ())), preferred_element_type=jnp.float32)


def kernel(
    tokens, gain, w_query, w_key, w_value, w_out, out, logs,
    raw, gains, gift, toks, weights, whole_out, queries, near, middle, wide, bias,
    combined, arrived, log_rows, both_logs, own_sem, send_sem, recv_sem,
):
    s, x = lax.axis_index("sp"), lax.axis_index("tp")
    core, chip = lax.rem(s, 2), lax.div(s, 2)
    y, z = lax.rem(chip, 4), lax.div(chip, 4)

    def turn(value, by):
        return lax.rem(value + (by + 4), 4)

    def spot(y_at, z_at, core_at):
        return (z_at * 4 + y_at) * 2 + core_at

    zp, zm, xp, xm = (turn(v, d) for v in (z, x) for d in (1, -1))
    line = lax.rem(y, 2)
    pair_y, apart_y = y + 1 - 2 * line, turn(y, 2 * line - 1)
    share = lax.rem(lax.div(y + 1, 2), 2)
    other = 1 - core
    partner = (spot(y, z, other), x)
    z_plus, z_minus = (spot(y, zp, core), x), (spot(y, zm, core), x)
    x_plus, x_minus = (s, xp), (s, xm)
    upper = lax.div(y, 2)
    later = (spot(3 - y, turn(z, upper), core), x)
    head = 2 * x + core

    crowd = []
    for flip_line in (0, 1):
        for flip_core in (0, 1):
            for step in range(4):
                if flip_line or flip_core or step:
                    y_at = pair_y if flip_line else y
                    core_at = other if flip_core else core
                    crowd.append((flip_line, flip_core, step, (spot(y_at, z, core_at), turn(x, step))))
    y_pair, y_apart = (spot(pair_y, z, core), x), (spot(apart_y, z, core), x)
    greeted = [partner, x_plus, x_minus, y_pair, y_apart, z_plus, z_minus]

    barrier = pltpu.get_barrier_semaphore()
    for device in greeted:
        pl.semaphore_signal(barrier, inc=1, device_id=device, device_id_type=MESH)

    counts, opened = [0], [0]

    def tiles_of(ref):
        return math.prod(ref.shape) * ref.dtype.itemsize // 4096

    def shape_of(count):
        for across_at in range(10, 0, -1):
            if count % across_at == 0 and count // across_at <= WIDTH // 16:
                return count // across_at, across_at
        return None

    def extent(count):
        down, over = shape_of(count)
        return weights.at[: down * 16, : over * HEAD_WIDTH]

    class Transfer:
        def __init__(self):
            self.index = opened[0]
            opened[0] += 1
            self.count = 0

        def begin(self, src, dst, device):
            count = tiles_of(src)
            if counts[-1] >= 520 and shape_of(counts[-1]):
                counts.append(0)
            counts[-1] += count
            self.count += count
            pltpu.make_async_remote_copy(
                src_ref=src, dst_ref=dst, send_sem=send_sem.at[len(counts) - 1],
                recv_sem=recv_sem.at[self.index], device_id=device, device_id_type=MESH,
            ).start()

        def arrive(self):
            self.done = True
            whole = extent(self.count)
            pltpu.make_async_copy(whole, whole, recv_sem.at[self.index]).wait()

    def send(src, dst, device):
        transfer = Transfer()
        transfer.begin(src, dst, device)
        return transfer

    def weight_rows(s_at, unit, first=0, count=PIECE):
        left, right = UNITS[unit]
        return weights.at[pl.ds(pl.multiple_of(s_at * PIECE + first, 16), count), left:right]

    def token_rows(line_at, core_at, x_at, b):
        return toks.at[x_at, b, line_at * 2 + core_at]

    take_tokens = pltpu.make_async_copy(tokens, raw, own_sem.at[0])
    take_gain = pltpu.make_async_copy(gain, gains, own_sem.at[1])
    take_tokens.start()
    take_gain.start()
    parts = [(w, group) for group in (2, 1) for w in (w_key, w_value)] + [(w_out, None)]
    parts += [(w_key, 0), (w_value, 0)] + [(w_query, group) for group in (2, 1, 0)]
    rows = pl.ds(pl.multiple_of(s * PIECE, PIECE), PIECE)

    def part_of(index, core_at):
        w, group = parts[index]
        lanes = pl.ds(pl.multiple_of(core_at * HEAD_WIDTH, HEAD_WIDTH), HEAD_WIDTH)
        src = w.at[:, lanes] if group is None else w.at[group, :, lanes]
        return src, weights.at[rows, index * HEAD_WIDTH : (index + 1) * HEAD_WIDTH]

    for index in range(10):
        pltpu.make_async_copy(*part_of(index, core), own_sem.at[2 + index // 5]).start()

    def normed(b):
        return rms_normed(raw[b].astype(jnp.float32), gains[...])

    take_tokens.wait()
    take_gain.wait()
    for b in range(SHARE):
        toks[x, b, line * 2 + core] = normed(share * SHARE + b)
    for b in range(SHARE):
        gift[b] = normed((1 - share) * SHARE + b)

    pl.semaphore_wait(barrier, len(greeted))

    swap = []
    for unit in (0, 1):
        swap.append(Transfer())
        for index in range(5 * unit, 5 * unit + 5):
            src, dst = part_of(index, other)
            swap[unit].begin(src, dst, partner)

    class Ring:
        def __init__(self, rows_of, first, second, names, cut):
            self.rows_of, self.first, self.second, self.cut = rows_of, first, second, cut
            self.names = names
            rows = rows_of(0)
            to_second, to_first = send(rows, rows, second), send(rows, rows, first)
            along_y = names[0] == "pair"
            self.from_first = to_first if along_y else to_second
            self.from_second = to_second if along_y else to_first
            self.on = []

        def pass_first(self):
            self.from_first.arrive()
            if self.cut < PIECE:
                rows = self.rows_of(self.names[0], self.cut, PIECE - self.cut)
                self.on.append(send(rows, rows, self.second))

        def pass_second(self):
            self.from_second.arrive()
            if self.cut > 0:
                rows = self.rows_of(self.names[1], 0, self.cut)
                self.on.append(send(rows, rows, self.first))

        def far(self):
            for copy in self.on:
                copy.arrive()

    ys = {0: y, "pair": pair_y, "apart": apart_y, "far": turn(y, 2)}
    zs = {0: z, -1: zm, 1: zp, 2: turn(z, 2)}

    def y_ring(dz, core_at, unit):
        return Ring(
            lambda step, *cut: weight_rows(spot(ys[step], zs[dz], core_at), unit, *cut),
            y_pair, y_apart, ("pair", "apart"), Y_CUT[unit],
        )

    def z_ring(dy, core_at, unit):
        return Ring(
            lambda step, *cut: weight_rows(spot(ys[dy], zs[step], core_at), unit, *cut),
            z_minus, z_plus, (-1, 1), Z_CUT[unit],
        )

    events = {}

    across = {step: Transfer() for step in (0, -1, 1, 2)}
    lines = (line, 1 - line)
    give, up, down, far_up, far_down = {}, {}, {}, {}, {}

    def cross(step, which, b):
        rows = token_rows(lines[which], core, turn(x, step), b)
        across[step].begin(rows, rows, partner)

    def launch(which, b):
        if which == 1:
            give[b].arrive()
        rows = token_rows(lines[which], core, x, b)
        up[which, b] = send(rows, rows, x_plus)
        down[which, b] = send(rows, rows, x_minus)
        cross(0, which, b)

    def onward(which, step, b):
        (up if step == -1 else down)[which, b].arrive()
        rows = token_rows(lines[which], core, turn(x, step), b)
        if (which, step) == (0, -1):
            far_up[b] = send(rows, rows, x_plus)
        if (which, step) == (1, 1):
            far_down[b] = send(rows, rows, x_minus)
        cross(step, which, b)

    def arrive_far(which, b):
        (far_up, far_down)[which][b].arrive()
        cross(2, which, b)

    def present(b):
        give[b] = send(gift.at[b], token_rows(line, core, x, b), y_pair)

    for b in range(SHARE):
        events[f"G{b}"] = functools.partial(present, b)
        for which in (0, 1):
            events[f"t0{b}" if which == 0 else f"g{b}"] = functools.partial(launch, which, b)
            events[f"up{which}{b}"] = functools.partial(onward, which, -1, b)
            events[f"dn{which}{b}"] = functools.partial(onward, which, 1, b)
            events[f"fu{b}" if which == 0 else f"fd{b}"] = functools.partial(arrive_far, which, b)

    def weight_events(unit):
        rings = {}

        def event(name):
            def keep(work):
                events[name + str(unit)] = work
            return keep

        def over_z(letter, dy):
            ring = rings["z" + letter] = z_ring(dy, core, unit)
            events[f"Zm{letter}{unit}"], events[f"Zp{letter}{unit}"] = ring.pass_first, ring.pass_second

        def over_y(letter, dz):
            ring = rings["y" + letter] = y_ring(dz, other, unit)
            events[f"Yp{letter}{unit}"], events[f"Ya{letter}{unit}"] = ring.pass_first, ring.pass_second

        @event("O")
        def _():
            whole = weight_rows(s, unit)
            pltpu.make_async_copy(whole, whole, own_sem.at[2 + unit]).wait()
            rings["O"] = y_ring(0, core, unit)
            over_z("0", 0)

        @event("R")
        def _():
            swap[unit].arrive()
            rings["R"] = z_ring(0, other, unit)
            over_y("0", 0)

        @event("Op")
        def _():
            rings["O"].pass_first()
            over_z("p", "pair")

        @event("Oa")
        def _():
            rings["O"].pass_second()
            over_z("a", "apart")

        @event("Of")
        def _():
            rings["O"].far()
            over_z("f", "far")

        @event("Rm")
        def _():
            rings["R"].pass_first()
            over_y("m", -1)

        @event("Rp")
        def _():
            rings["R"].pass_second()
            over_y("p", 1)

        @event("Rf")
        def _():
            rings["R"].far()
            over_y("f", 2)

        @event("W")
        def _():
            for letter in "0paf":
                rings["z" + letter].far()
            for letter in "0mpf":
                rings["y" + letter].far()

    weight_events(0)
    weight_events(1)

    def project(x_at, left, width):
        rows = toks[x_at].reshape(SHARE * BLOCKS * 32, WIDTH)
        return dot(rows, weights[:, left : left + width]).astype(jnp.bfloat16)

    def block_rows(x_at):
        return pl.ds(pl.multiple_of(x_at * 32, 32), 32)

    def lay(found, left, buffer, x_at, ahead):
        part = found[:, left : left + HEAD_WIDTH].reshape(SHARE, BLOCKS, 32, HEAD_WIDTH)
        buffer[:, ahead : ahead + BLOCKS, block_rows(x_at), :] = part

    def keys_of(step):
        x_at = turn(x, step)
        across[step].arrive()
        for place, (keys, group) in enumerate(((wide, 2), (middle, 1))):
            found = project(x_at, place * 2 * HEAD_WIDTH, 2 * HEAD_WIDTH)
            for which in (0, 1):
                lay(found, which * HEAD_WIDTH, keys.at[which], x_at, AHEAD[group])

    halo = []

    def pass_on(keys, group, x_at, share_at):
        ahead = AHEAD[group]
        halo.append(
            send(
                keys.at[:, share_at, BLOCKS:, block_rows(x_at), :],
                keys.at[:, share_at, :ahead, block_rows(x_at), :],
                later,
            )
        )

    def pass_all(step):
        for keys, group in ((wide, 2), (middle, 1)):
            pass_on(keys, group, turn(x, step), slice(None))

    def head_columns(x_at, core_at, half=None):
        lanes = pl.ds(pl.multiple_of((2 * x_at + core_at) * HEAD_WIDTH, HEAD_WIDTH), HEAD_WIDTH)
        if half is None:
            return whole_out.at[:, lanes]
        return whole_out.at[pl.ds(half * (WIDTH // 2), WIDTH // 2), lanes]

    out_swap = []

    out_way = {}

    def out_event(name):
        def keep(work):
            events[name] = work
        return keep

    def out_cross(rows):
        out_swap.append(send(rows, rows, partner))

    @out_event("o0")
    def _():
        out_rows = weights.at[:, 4 * HEAD_WIDTH : 5 * HEAD_WIDTH]
        mine = head_columns(x, core)
        out_way["up"] = send(out_rows, mine, x_plus)
        out_way["down"] = send(out_rows, mine, x_minus)
        out_swap.append(send(out_rows, mine, partner))
        lanes = pl.ds(pl.multiple_of(head * HEAD_WIDTH, HEAD_WIDTH), HEAD_WIDTH)
        whole_out[:, lanes] = weights[:, 4 * HEAD_WIDTH : 5 * HEAD_WIDTH]

    @out_event("oum")
    def _():
        out_way["up"].arrive()
        rows = head_columns(xm, core, 0)
        out_way["far_up"] = send(rows, rows, x_plus)
        out_cross(head_columns(xm, core))

    @out_event("odm")
    def _():
        out_way["down"].arrive()
        rows = head_columns(xp, core, 1)
        out_way["far_down"] = send(rows, rows, x_minus)
        out_cross(head_columns(xp, core))

    @out_event("ofu")
    def _():
        out_way["far_up"].arrive()
        out_cross(head_columns(turn(x, 2), core, 0))

    @out_event("ofd")
    def _():
        out_way["far_down"].arrive()
        out_cross(head_columns(turn(x, 2), core, 1))

    near[:, :, 0, :96, :] = jnp.zeros((2, SHARE, 96, HEAD_WIDTH), jnp.bfloat16)
    log_rows[...] = jnp.zeros_like(log_rows)
    left = 0
    for ahead, window, dilation in zip(AHEAD, WINDOW, (1, DILATION_MIDDLE, DILATION_WIDE)):
        query_at = lax.broadcasted_iota(jnp.int32, (BLOCK, window), 0)
        key_at = lax.broadcasted_iota(jnp.int32, (BLOCK, window), 1)
        lag = query_at + ahead * BLOCK - key_at
        allowed = (lag >= 0) & (lag <= STEPS * dilation) & ((lag & (dilation - 1)) == 0)
        bias[:, left : left + window] = jnp.where(allowed, jnp.float32(0), jnp.float32(ABSENT))
        left += window

    def keys_near(x_at, carry):
        found = project(x_at, UNITS[1][0], 2 * HEAD_WIDTH)
        for which in (0, 1):
            lay(found, which * HEAD_WIDTH, near.at[which], x_at, AHEAD[0])
        return carry

    def ask(x_at, carry):
        left = UNITS[1][0] + 2 * HEAD_WIDTH
        found = project(x_at, left, 2 * HEAD_WIDTH)
        lay(found, 0, queries.at[2], x_at, 0)
        lay(found, HEAD_WIDTH, queries.at[1], x_at, 0)
        lay(project(x_at, left + 2 * HEAD_WIDTH, HEAD_WIDTH), 0, queries.at[0], x_at, 0)
        return carry

    def early_keys(step):
        keys_of(step)
        pass_all(step)

    for letter, step in (("0", 0), ("m", -1), ("p", 1)):
        events["K" + letter] = functools.partial(early_keys, step)

    @out_event("K2")
    def _():
        keys_of(2)
        for b in range(SHARE):
            for keys, group in ((wide, 2), (middle, 1)):
                pass_on(keys, group, turn(x, 2), pl.ds(b, 1))

    @out_event("N")
    def _():
        lax.fori_loop(0, 4, keys_near, 0)
        halo.append(send(near.at[:, :, BLOCKS, 96:, :], near.at[:, :, 0, 96:, :], later))

    @out_event("Q")
    def _():
        lax.fori_loop(0, 4, ask, 0)

    for name in ORDER:
        events[name]()

    factor = math.log2(math.e) / math.sqrt(HEAD_WIDTH)
    start_at = (z * 2 + upper) * ROWS
    lanes = pl.ds(pl.multiple_of(head * HEAD_WIDTH, HEAD_WIDTH), HEAD_WIDTH)

    def attend(b, block):
        scores, left = [], 0
        for group, keys in enumerate((near, middle, wide)):
            window = WINDOW[group]
            seen = keys[0, b, block : block + AHEAD[group] + 1].reshape(window, HEAD_WIDTH)
            score = dot_t(queries[group, b, block], seen)
            first = start_at + (block - AHEAD[group]) * BLOCK
            hidden = bias[:, left : left + window]
            if block < AHEAD[group]:
                key_at = lax.broadcasted_iota(jnp.int32, (1, window), 1) + first
                hidden = hidden + jnp.where(key_at >= 0, jnp.float32(0), jnp.float32(ABSENT))
            scores.append(score * factor + hidden)
            left += window
        peak = functools.reduce(
            jnp.maximum, [jnp.max(score, axis=1, keepdims=True) for score in scores]
        )
        total, mixed = 0.0, 0.0
        for group, keys in enumerate((near, middle, wide)):
            lifted = jnp.exp2(scores[group] - peak)
            total = total + jnp.sum(lifted, axis=1, keepdims=True)
            seen = keys[1, b, block : block + AHEAD[group] + 1].reshape(WINDOW[group], HEAD_WIDTH)
            mixed = mixed + dot(lifted.astype(jnp.bfloat16), seen)
        combined[b, block * BLOCK : (block + 1) * BLOCK, :] = (mixed / total).astype(jnp.bfloat16)
        log = (peak + jnp.log2(total)) * math.log(2.0)
        log_rows[block, b : b + 1, :] = jnp.transpose(jnp.broadcast_to(log, (BLOCK, BLOCK)))[0:1, :]

    def rows_for(line_at, core_at, x_at):
        return pl.ds(pl.multiple_of(line_at * 256 + core_at * 128 + x_at * 32, 32), 32)

    for b in range(SHARE):
        attend(b, BLOCKS - 1)
    events["ofu"]()
    events["ofd"]()
    for copy in halo[:6] + halo[12:]:
        copy.arrive()
    exchange = Transfer()
    for b in range(SHARE):
        halo[6 + 2 * b].arrive()
        halo[7 + 2 * b].arrive()
        for block in range(BLOCKS - 1):
            attend(b, block)

        for flip_line, flip_core, step, device in crowd:
            line_at = 1 - line if flip_line else line
            core_at = other if flip_core else core
            exchange.begin(
                combined.at[b, rows_for(line_at, core_at, turn(x, step)), :],
                arrived.at[share * SHARE + b, :, lanes],
                device,
            )
            if step == 0 and b == SHARE - 1:
                exchange.begin(
                    log_rows.at[line_at * 2 + core_at], both_logs.at[core, share], device
                )
        arrived[share * SHARE + b, :, lanes] = combined[b, rows_for(line, core, x), :]
    both_logs[core, share] = log_rows[line * 2 + core]
    for copy in out_swap + [exchange]:
        copy.arrive()

    everything = arrived[...].reshape(192, HEADS * HEAD_WIDTH)
    for tile in range(8):
        part = dot_t(everything, whole_out[tile * 256 : (tile + 1) * 256, :]).astype(jnp.bfloat16)
        out[:, :, tile * 256 : (tile + 1) * 256] = part.reshape(BATCH, 32, 256)
    for core_at in range(2):
        for share_at in range(2):
            for b in range(SHARE):
                logs[share_at * SHARE + b, core_at : core_at + 1, :] = both_logs[core_at, share_at, b : b + 1, :]

    assert opened[0] <= ARRIVALS and len(counts) <= SENDS, (opened, counts)
    for index, count in enumerate(counts):
        whole = extent(count)
        pltpu.make_async_copy(whole, whole, send_sem.at[index]).wait()


ARRIVALS = 130
SENDS = 8


def shards(tokens, norm_gain, w_query, w_key, w_value, w_out):
    bf16, f32 = jnp.bfloat16, jnp.float32
    operands = (
        jnp.transpose(tokens, (1, 0, 2)), norm_gain.reshape(1, WIDTH),
        w_query, w_key, w_value, jnp.transpose(w_out),
    )
    mixed, logs = pl.pallas_call(
        kernel,
        out_shape=(
            jax.ShapeDtypeStruct((BATCH, 32, WIDTH), bf16),
            jax.ShapeDtypeStruct((BATCH, 2, 128), f32),
        ),
        in_specs=[pl.BlockSpec(memory_space=pltpu.HBM)] * 6,
        out_specs=[pl.BlockSpec(memory_space=pltpu.VMEM)] * 2,
        scratch_shapes=[
            pltpu.VMEM((BATCH, 32, WIDTH), bf16),
            pltpu.VMEM((1, WIDTH), f32),
            pltpu.VMEM((SHARE, 32, WIDTH), bf16),
            pltpu.VMEM((4, SHARE, BLOCKS, 32, WIDTH), bf16),
            pltpu.VMEM((WIDTH, COLUMNS), bf16),
            pltpu.VMEM((WIDTH, HEADS * HEAD_WIDTH), bf16),
            pltpu.VMEM((GROUPS, SHARE, BLOCKS, BLOCK, HEAD_WIDTH), bf16),
            pltpu.VMEM((2, SHARE, AHEAD[0] + BLOCKS, BLOCK, HEAD_WIDTH), bf16),
            pltpu.VMEM((2, SHARE, AHEAD[1] + BLOCKS, BLOCK, HEAD_WIDTH), bf16),
            pltpu.VMEM((2, SHARE, AHEAD[2] + BLOCKS, BLOCK, HEAD_WIDTH), bf16),
            pltpu.VMEM((BLOCK, KEYS), f32),
            pltpu.VMEM((SHARE, ROWS, HEAD_WIDTH), bf16),
            pltpu.VMEM((BATCH, 32, HEADS * HEAD_WIDTH), bf16),
            pltpu.VMEM((4, 8, 128), f32),
            pltpu.VMEM((2, 2, 8, 128), f32),
            pltpu.SemaphoreType.DMA((4,)),
            pltpu.SemaphoreType.DMA((SENDS,)),
            pltpu.SemaphoreType.DMA((ARRIVALS,)),
        ],
        compiler_params=pltpu.CompilerParams(
            collective_id=0, has_side_effects=True, vmem_limit_bytes=44 * 1024 * 1024
        ),
    )(*(pltpu.with_memory_space_constraint(array, pltpu.HBM) for array in operands))
    return (jnp.transpose(mixed, (1, 0, 2)), jnp.transpose(logs, (2, 0, 1)))


def solution(mesh):
    in_specs = (
        P(("sp", "tp"), None, None),
        P(),
        P(None, "sp", "tp"),
        P(None, "sp", "tp"),
        P(None, "sp", "tp"),
        P("tp", "sp"),
    )
    out_specs = (P(("sp", "tp"), None, None), P("sp", None, "tp"))
    return jax.shard_map(shards, mesh=mesh, in_specs=in_specs, out_specs=out_specs, check_vma=False)
```

```python
import functools
import math

import jax
import jax.numpy as jnp
from jax import lax
from jax.experimental import pallas as pl
from jax.experimental.pallas import tpu as pltpu
from jax.sharding import PartitionSpec as P

GROUPS = 3
HEADS = 8
HEAD_WIDTH = 128
STEPS = 24
DILATION_MIDDLE = 4
DILATION_WIDE = 16
WIDTH = 2048
BATCH = 6
SHARE = BATCH // 2
ROWS = 512
AHEAD = (1, 1, 3)
BLOCK = 128
BLOCKS = ROWS // BLOCK
WINDOW = tuple((ahead + 1) * BLOCK for ahead in AHEAD)
KEYS = sum(WINDOW)
PIECE = 64
COLUMNS = 10 * HEAD_WIDTH
UNITS = ((0, 5 * HEAD_WIDTH), (5 * HEAD_WIDTH, 10 * HEAD_WIDTH))
ABSENT = -1e30
ORDER = (
    "t00", "O0", "G0", "t01", "t02", "R0", "G1", "G2", "Op0", "Oa0", "Zm00", "Zp00", "up00",
    "dn00", "Rm0", "Rp0", "Ya00", "g0", "up01", "dn01", "Zmp0", "Zpp0", "Yp00", "Zma0",
    "Zpa0", "Yam0", "O1", "up02", "dn02", "g1", "Rf0", "Yap0", "dn10", "fu0", "R1", "Of0",
    "g2", "Zm01", "Zp01", "Oa1", "Ypm0", "up10", "dn11", "Yaf0", "Ypp0", "Rm1", "fu1", "Rp1",
    "fd0", "Zmf0", "Zpf0", "Op1", "Ya01", "Ypf0", "fu2", "dn12", "Zma1", "Zpa1", "Yp01",
    "Rf1", "Yam1", "up11", "fd1", "Of1", "Yap1", "Zmp1", "Zpp1", "Ypm1", "W0", "o0", "K0",
    "up12", "fd2", "Ypp1", "Yaf1", "Zmf1", "Zpf1", "Km", "Ypf1", "Kp", "K2", "oum", "odm",
    "W1", "N", "Q",
)
Y_CUT = (16, 64)
Z_CUT = (48, 48)

epsilon = 1e-06
MESH = pl.DeviceIdType.MESH


def rms_normed(widened, gain):
    scaled = widened * lax.rsqrt(jnp.mean(widened * widened, axis=-1, keepdims=True) + epsilon)
    return (scaled * gain).astype(jnp.bfloat16)


def dot(a, b):
    return lax.dot_general(a, b, (((1,), (0,)), ((), ())), preferred_element_type=jnp.float32)


def dot_t(a, b):
    return lax.dot_general(a, b, (((1,), (1,)), ((), ())), preferred_element_type=jnp.float32)


def kernel(
    tokens, gain, w_query, w_key, w_value, w_out, out, logs,
    raw, gains, gift, toks, weights, whole_out, queries, near, middle, wide, bias,
    combined, arrived, log_rows, both_logs, own_sem, send_sem, recv_sem,
):
    s, x = lax.axis_index("sp"), lax.axis_index("tp")
    core, chip = lax.rem(s, 2), lax.div(s, 2)
    y, z = lax.rem(chip, 4), lax.div(chip, 4)

    def turn(value, by):
        return lax.rem(value + (by + 4), 4)

    def spot(y_at, z_at, core_at):
        return (z_at * 4 + y_at) * 2 + core_at

    zp, zm, xp, xm = (turn(v, d) for v in (z, x) for d in (1, -1))
    line = lax.rem(y, 2)
    pair_y, apart_y = y + 1 - 2 * line, turn(y, 2 * line - 1)
    share = lax.rem(lax.div(y + 1, 2), 2)
    other = 1 - core
    partner = (spot(y, z, other), x)
    z_plus, z_minus = (spot(y, zp, core), x), (spot(y, zm, core), x)
    x_plus, x_minus = (s, xp), (s, xm)
    upper = lax.div(y, 2)
    later = (spot(3 - y, turn(z, upper), core), x)
    head = 2 * x + core

    crowd = []
    for flip_line in (0, 1):
        for flip_core in (0, 1):
            for step in range(4):
                if flip_line or flip_core or step:
                    y_at = pair_y if flip_line else y
                    core_at = other if flip_core else core
                    crowd.append((flip_line, flip_core, step, (spot(y_at, z, core_at), turn(x, step))))
    y_pair, y_apart = (spot(pair_y, z, core), x), (spot(apart_y, z, core), x)
    greeted = [partner, x_plus, x_minus, y_pair, y_apart, z_plus, z_minus]

    barrier = pltpu.get_barrier_semaphore()
    for device in greeted:
        pl.semaphore_signal(barrier, inc=1, device_id=device, device_id_type=MESH)

    counts, opened = [0], [0]

    def tiles_of(ref):
        return math.prod(ref.shape) * ref.dtype.itemsize // 4096

    def shape_of(count):
        for across_at in range(10, 0, -1):
            if count % across_at == 0 and count // across_at <= WIDTH // 16:
                return count // across_at, across_at
        return None

    def extent(count):
        down, over = shape_of(count)
        return weights.at[: down * 16, : over * HEAD_WIDTH]

    class Transfer:
        def __init__(self):
            self.index = opened[0]
            opened[0] += 1
            self.count = 0

        def begin(self, src, dst, device):
            count = tiles_of(src)
            if counts[-1] >= 520 and shape_of(counts[-1]):
                counts.append(0)
            counts[-1] += count
            self.count += count
            pltpu.make_async_remote_copy(
                src_ref=src, dst_ref=dst, send_sem=send_sem.at[len(counts) - 1],
                recv_sem=recv_sem.at[self.index], device_id=device, device_id_type=MESH,
            ).start()

        def arrive(self):
            self.done = True
            whole = extent(self.count)
            pltpu.make_async_copy(whole, whole, recv_sem.at[self.index]).wait()

    def send(src, dst, device):
        transfer = Transfer()
        transfer.begin(src, dst, device)
        return transfer

    def weight_rows(s_at, unit, first=0, count=PIECE):
        left, right = UNITS[unit]
        return weights.at[pl.ds(pl.multiple_of(s_at * PIECE + first, 16), count), left:right]

    def token_rows(line_at, core_at, x_at, b):
        return toks.at[x_at, b, line_at * 2 + core_at]

    take_tokens = pltpu.make_async_copy(tokens, raw, own_sem.at[0])
    take_gain = pltpu.make_async_copy(gain, gains, own_sem.at[1])
    take_tokens.start()
    take_gain.start()
    parts = [(w, group) for group in (2, 1) for w in (w_key, w_value)] + [(w_out, None)]
    parts += [(w_key, 0), (w_value, 0)] + [(w_query, group) for group in (2, 1, 0)]
    rows = pl.ds(pl.multiple_of(s * PIECE, PIECE), PIECE)

    def part_of(index, core_at):
        w, group = parts[index]
        lanes = pl.ds(pl.multiple_of(core_at * HEAD_WIDTH, HEAD_WIDTH), HEAD_WIDTH)
        src = w.at[:, lanes] if group is None else w.at[group, :, lanes]
        return src, weights.at[rows, index * HEAD_WIDTH : (index + 1) * HEAD_WIDTH]

    for index in range(10):
        pltpu.make_async_copy(*part_of(index, core), own_sem.at[2 + index // 5]).start()

    def normed(b):
        return rms_normed(raw[b].astype(jnp.float32), gains[...])

    take_tokens.wait()
    take_gain.wait()
    for b in range(SHARE):
        toks[x, b, line * 2 + core] = normed(share * SHARE + b)
    for b in range(SHARE):
        gift[b] = normed((1 - share) * SHARE + b)

    pl.semaphore_wait(barrier, len(greeted))

    swap = []
    for unit in (0, 1):
        swap.append(Transfer())
        for index in range(5 * unit, 5 * unit + 5):
            src, dst = part_of(index, other)
            swap[unit].begin(src, dst, partner)

    class Ring:
        def __init__(self, rows_of, first, second, names, cut):
            self.rows_of, self.first, self.second, self.cut = rows_of, first, second, cut
            self.names = names
            rows = rows_of(0)
            to_second, to_first = send(rows, rows, second), send(rows, rows, first)
            along_y = names[0] == "pair"
            self.from_first = to_first if along_y else to_second
            self.from_second = to_second if along_y else to_first
            self.on = []

        def pass_first(self):
            self.from_first.arrive()
            if self.cut < PIECE:
                rows = self.rows_of(self.names[0], self.cut, PIECE - self.cut)
                self.on.append(send(rows, rows, self.second))

        def pass_second(self):
            self.from_second.arrive()
            if self.cut > 0:
                rows = self.rows_of(self.names[1], 0, self.cut)
                self.on.append(send(rows, rows, self.first))

        def far(self):
            for copy in self.on:
                copy.arrive()

    ys = {0: y, "pair": pair_y, "apart": apart_y, "far": turn(y, 2)}
    zs = {0: z, -1: zm, 1: zp, 2: turn(z, 2)}

    def y_ring(dz, core_at, unit):
        return Ring(
            lambda step, *cut: weight_rows(spot(ys[step], zs[dz], core_at), unit, *cut),
            y_pair, y_apart, ("pair", "apart"), Y_CUT[unit],
        )

    def z_ring(dy, core_at, unit):
        return Ring(
            lambda step, *cut: weight_rows(spot(ys[dy], zs[step], core_at), unit, *cut),
            z_minus, z_plus, (-1, 1), Z_CUT[unit],
        )

    events = {}

    across = {step: Transfer() for step in (0, -1, 1, 2)}
    lines = (line, 1 - line)
    give, up, down, far_up, far_down = {}, {}, {}, {}, {}

    def cross(step, which, b):
        rows = token_rows(lines[which], core, turn(x, step), b)
        across[step].begin(rows, rows, partner)

    def launch(which, b):
        if which == 1:
            give[b].arrive()
        rows = token_rows(lines[which], core, x, b)
        up[which, b] = send(rows, rows, x_plus)
        down[which, b] = send(rows, rows, x_minus)
        cross(0, which, b)

    def onward(which, step, b):
        (up if step == -1 else down)[which, b].arrive()
        rows = token_rows(lines[which], core, turn(x, step), b)
        if (which, step) == (0, -1):
            far_up[b] = send(rows, rows, x_plus)
        if (which, step) == (1, 1):
            far_down[b] = send(rows, rows, x_minus)
        cross(step, which, b)

    def arrive_far(which, b):
        (far_up, far_down)[which][b].arrive()
        cross(2, which, b)

    def present(b):
        give[b] = send(gift.at[b], token_rows(line, core, x, b), y_pair)

    for b in range(SHARE):
        events[f"G{b}"] = functools.partial(present, b)
        for which in (0, 1):
            events[f"t0{b}" if which == 0 else f"g{b}"] = functools.partial(launch, which, b)
            events[f"up{which}{b}"] = functools.partial(onward, which, -1, b)
            events[f"dn{which}{b}"] = functools.partial(onward, which, 1, b)
            events[f"fu{b}" if which == 0 else f"fd{b}"] = functools.partial(arrive_far, which, b)

    def weight_events(unit):
        rings = {}

        def event(name):
            def keep(work):
                events[name + str(unit)] = work
            return keep

        def over_z(letter, dy):
            ring = rings["z" + letter] = z_ring(dy, core, unit)
            events[f"Zm{letter}{unit}"], events[f"Zp{letter}{unit}"] = ring.pass_first, ring.pass_second

        def over_y(letter, dz):
            ring = rings["y" + letter] = y_ring(dz, other, unit)
            events[f"Yp{letter}{unit}"], events[f"Ya{letter}{unit}"] = ring.pass_first, ring.pass_second

        @event("O")
        def _():
            whole = weight_rows(s, unit)
            pltpu.make_async_copy(whole, whole, own_sem.at[2 + unit]).wait()
            rings["O"] = y_ring(0, core, unit)
            over_z("0", 0)

        @event("R")
        def _():
            swap[unit].arrive()
            rings["R"] = z_ring(0, other, unit)
            over_y("0", 0)

        @event("Op")
        def _():
            rings["O"].pass_first()
            over_z("p", "pair")

        @event("Oa")
        def _():
            rings["O"].pass_second()
            over_z("a", "apart")

        @event("Of")
        def _():
            rings["O"].far()
            over_z("f", "far")

        @event("Rm")
        def _():
            rings["R"].pass_first()
            over_y("m", -1)

        @event("Rp")
        def _():
            rings["R"].pass_second()
            over_y("p", 1)

        @event("Rf")
        def _():
            rings["R"].far()
            over_y("f", 2)

        @event("W")
        def _():
            for letter in "0paf":
                rings["z" + letter].far()
            for letter in "0mpf":
                rings["y" + letter].far()

    weight_events(0)
    weight_events(1)

    def project(x_at, left, width):
        rows = toks[x_at].reshape(SHARE * BLOCKS * 32, WIDTH)
        return dot(rows, weights[:, left : left + width]).astype(jnp.bfloat16)

    def block_rows(x_at):
        return pl.ds(pl.multiple_of(x_at * 32, 32), 32)

    def lay(found, left, buffer, x_at, ahead):
        part = found[:, left : left + HEAD_WIDTH].reshape(SHARE, BLOCKS, 32, HEAD_WIDTH)
        buffer[:, ahead : ahead + BLOCKS, block_rows(x_at), :] = part

    def keys_of(step):
        x_at = turn(x, step)
        across[step].arrive()
        for place, (keys, group) in enumerate(((wide, 2), (middle, 1))):
            found = project(x_at, place * 2 * HEAD_WIDTH, 2 * HEAD_WIDTH)
            for which in (0, 1):
                lay(found, which * HEAD_WIDTH, keys.at[which], x_at, AHEAD[group])

    halo = []

    def pass_on(keys, group, x_at, share_at):
        ahead = AHEAD[group]
        halo.append(
            send(
                keys.at[:, share_at, BLOCKS:, block_rows(x_at), :],
                keys.at[:, share_at, :ahead, block_rows(x_at), :],
                later,
            )
        )

    def pass_all(step):
        for keys, group in ((wide, 2), (middle, 1)):
            pass_on(keys, group, turn(x, step), slice(None))

    def head_columns(x_at, core_at, half=None):
        lanes = pl.ds(pl.multiple_of((2 * x_at + core_at) * HEAD_WIDTH, HEAD_WIDTH), HEAD_WIDTH)
        if half is None:
            return whole_out.at[:, lanes]
        return whole_out.at[pl.ds(half * (WIDTH // 2), WIDTH // 2), lanes]

    out_swap = []

    out_way = {}

    def out_event(name):
        def keep(work):
            events[name] = work
        return keep

    def out_cross(rows):
        out_swap.append(send(rows, rows, partner))

    @out_event("o0")
    def _():
        out_rows = weights.at[:, 4 * HEAD_WIDTH : 5 * HEAD_WIDTH]
        mine = head_columns(x, core)
        out_way["up"] = send(out_rows, mine, x_plus)
        out_way["down"] = send(out_rows, mine, x_minus)
        out_swap.append(send(out_rows, mine, partner))
        lanes = pl.ds(pl.multiple_of(head * HEAD_WIDTH, HEAD_WIDTH), HEAD_WIDTH)
        whole_out[:, lanes] = weights[:, 4 * HEAD_WIDTH : 5 * HEAD_WIDTH]

    @out_event("oum")
    def _():
        out_way["up"].arrive()
        rows = head_columns(xm, core, 0)
        out_way["far_up"] = send(rows, rows, x_plus)
        out_cross(head_columns(xm, core))

    @out_event("odm")
    def _():
        out_way["down"].arrive()
        rows = head_columns(xp, core, 1)
        out_way["far_down"] = send(rows, rows, x_minus)
        out_cross(head_columns(xp, core))

    @out_event("ofu")
    def _():
        out_way["far_up"].arrive()
        out_cross(head_columns(turn(x, 2), core, 0))

    @out_event("ofd")
    def _():
        out_way["far_down"].arrive()
        out_cross(head_columns(turn(x, 2), core, 1))

    near[:, :, 0, :96, :] = jnp.zeros((2, SHARE, 96, HEAD_WIDTH), jnp.bfloat16)
    log_rows[...] = jnp.zeros_like(log_rows)
    left = 0
    for ahead, window, dilation in zip(AHEAD, WINDOW, (1, DILATION_MIDDLE, DILATION_WIDE)):
        query_at = lax.broadcasted_iota(jnp.int32, (BLOCK, window), 0)
        key_at = lax.broadcasted_iota(jnp.int32, (BLOCK, window), 1)
        lag = query_at + ahead * BLOCK - key_at
        allowed = (lag >= 0) & (lag <= STEPS * dilation) & ((lag & (dilation - 1)) == 0)
        bias[:, left : left + window] = jnp.where(allowed, jnp.float32(0), jnp.float32(ABSENT))
        left += window

    def keys_near(x_at, carry):
        found = project(x_at, UNITS[1][0], 2 * HEAD_WIDTH)
        for which in (0, 1):
            lay(found, which * HEAD_WIDTH, near.at[which], x_at, AHEAD[0])
        return carry

    def ask(x_at, carry):
        left = UNITS[1][0] + 2 * HEAD_WIDTH
        found = project(x_at, left, 2 * HEAD_WIDTH)
        lay(found, 0, queries.at[2], x_at, 0)
        lay(found, HEAD_WIDTH, queries.at[1], x_at, 0)
        lay(project(x_at, left + 2 * HEAD_WIDTH, HEAD_WIDTH), 0, queries.at[0], x_at, 0)
        return carry

    def early_keys(step):
        keys_of(step)
        pass_all(step)

    for letter, step in (("0", 0), ("m", -1), ("p", 1)):
        events["K" + letter] = functools.partial(early_keys, step)

    @out_event("K2")
    def _():
        keys_of(2)
        for b in range(SHARE):
            for keys, group in ((wide, 2), (middle, 1)):
                pass_on(keys, group, turn(x, 2), pl.ds(b, 1))

    @out_event("N")
    def _():
        lax.fori_loop(0, 4, keys_near, 0)
        halo.append(send(near.at[:, :, BLOCKS, 96:, :], near.at[:, :, 0, 96:, :], later))

    @out_event("Q")
    def _():
        lax.fori_loop(0, 4, ask, 0)

    for name in ORDER:
        events[name]()

    factor = math.log2(math.e) / math.sqrt(HEAD_WIDTH)
    start_at = (z * 2 + upper) * ROWS
    lanes = pl.ds(pl.multiple_of(head * HEAD_WIDTH, HEAD_WIDTH), HEAD_WIDTH)

    def attend(b, block):
        scores, left = [], 0
        for group, keys in enumerate((near, middle, wide)):
            window = WINDOW[group]
            seen = keys[0, b, block : block + AHEAD[group] + 1].reshape(window, HEAD_WIDTH)
            score = dot_t(queries[group, b, block], seen)
            first = start_at + (block - AHEAD[group]) * BLOCK
            hidden = bias[:, left : left + window]
            if block < AHEAD[group]:
                key_at = lax.broadcasted_iota(jnp.int32, (1, window), 1) + first
                hidden = hidden + jnp.where(key_at >= 0, jnp.float32(0), jnp.float32(ABSENT))
            scores.append(score * factor + hidden)
            left += window
        peak = functools.reduce(
            jnp.maximum, [jnp.max(score, axis=1, keepdims=True) for score in scores]
        )
        total, mixed = 0.0, 0.0
        for group, keys in enumerate((near, middle, wide)):
            lifted = jnp.exp2(scores[group] - peak)
            total = total + jnp.sum(lifted, axis=1, keepdims=True)
            seen = keys[1, b, block : block + AHEAD[group] + 1].reshape(WINDOW[group], HEAD_WIDTH)
            mixed = mixed + dot(lifted.astype(jnp.bfloat16), seen)
        combined[b, block * BLOCK : (block + 1) * BLOCK, :] = (mixed / total).astype(jnp.bfloat16)
        log = (peak + jnp.log2(total)) * math.log(2.0)
        log_rows[block, b : b + 1, :] = jnp.transpose(jnp.broadcast_to(log, (BLOCK, BLOCK)))[0:1, :]

    def rows_for(line_at, core_at, x_at):
        return pl.ds(pl.multiple_of(line_at * 256 + core_at * 128 + x_at * 32, 32), 32)

    for b in range(SHARE):
        attend(b, BLOCKS - 1)
    for copy in halo[:6] + halo[12:]:
        copy.arrive()
    exchange = Transfer()
    for b in range(SHARE):
        halo[6 + 2 * b].arrive()
        halo[7 + 2 * b].arrive()
        for block in range(BLOCKS - 1):
            attend(b, block)

        for flip_line, flip_core, step, device in crowd:
            line_at = 1 - line if flip_line else line
            core_at = other if flip_core else core
            exchange.begin(
                combined.at[b, rows_for(line_at, core_at, turn(x, step)), :],
                arrived.at[share * SHARE + b, :, lanes],
                device,
            )
            if step == 0 and b == SHARE - 1:
                exchange.begin(
                    log_rows.at[line_at * 2 + core_at], both_logs.at[core, share], device
                )
        arrived[share * SHARE + b, :, lanes] = combined[b, rows_for(line, core, x), :]
    both_logs[core, share] = log_rows[line * 2 + core]
    events["ofu"]()
    events["ofd"]()
    for copy in out_swap + [exchange]:
        copy.arrive()

    everything = arrived[...].reshape(192, HEADS * HEAD_WIDTH)
    for tile in range(8):
        part = dot_t(everything, whole_out[tile * 256 : (tile + 1) * 256, :]).astype(jnp.bfloat16)
        out[:, :, tile * 256 : (tile + 1) * 256] = part.reshape(BATCH, 32, 256)
    for core_at in range(2):
        for share_at in range(2):
            for b in range(SHARE):
                logs[share_at * SHARE + b, core_at : core_at + 1, :] = both_logs[core_at, share_at, b : b + 1, :]

    assert opened[0] <= ARRIVALS and len(counts) <= SENDS, (opened, counts)
    for index, count in enumerate(counts):
        whole = extent(count)
        pltpu.make_async_copy(whole, whole, send_sem.at[index]).wait()


ARRIVALS = 130
SENDS = 8


def shards(tokens, norm_gain, w_query, w_key, w_value, w_out):
    bf16, f32 = jnp.bfloat16, jnp.float32
    operands = (
        jnp.transpose(tokens, (1, 0, 2)), norm_gain.reshape(1, WIDTH),
        w_query, w_key, w_value, jnp.transpose(w_out),
    )
    mixed, logs = pl.pallas_call(
        kernel,
        out_shape=(
            jax.ShapeDtypeStruct((BATCH, 32, WIDTH), bf16),
            jax.ShapeDtypeStruct((BATCH, 2, 128), f32),
        ),
        in_specs=[pl.BlockSpec(memory_space=pltpu.HBM)] * 6,
        out_specs=[pl.BlockSpec(memory_space=pltpu.VMEM)] * 2,
        scratch_shapes=[
            pltpu.VMEM((BATCH, 32, WIDTH), bf16),
            pltpu.VMEM((1, WIDTH), f32),
            pltpu.VMEM((SHARE, 32, WIDTH), bf16),
            pltpu.VMEM((4, SHARE, BLOCKS, 32, WIDTH), bf16),
            pltpu.VMEM((WIDTH, COLUMNS), bf16),
            pltpu.VMEM((WIDTH, HEADS * HEAD_WIDTH), bf16),
            pltpu.VMEM((GROUPS, SHARE, BLOCKS, BLOCK, HEAD_WIDTH), bf16),
            pltpu.VMEM((2, SHARE, AHEAD[0] + BLOCKS, BLOCK, HEAD_WIDTH), bf16),
            pltpu.VMEM((2, SHARE, AHEAD[1] + BLOCKS, BLOCK, HEAD_WIDTH), bf16),
            pltpu.VMEM((2, SHARE, AHEAD[2] + BLOCKS, BLOCK, HEAD_WIDTH), bf16),
            pltpu.VMEM((BLOCK, KEYS), f32),
            pltpu.VMEM((SHARE, ROWS, HEAD_WIDTH), bf16),
            pltpu.VMEM((BATCH, 32, HEADS * HEAD_WIDTH), bf16),
            pltpu.VMEM((4, 8, 128), f32),
            pltpu.VMEM((2, 2, 8, 128), f32),
            pltpu.SemaphoreType.DMA((4,)),
            pltpu.SemaphoreType.DMA((SENDS,)),
            pltpu.SemaphoreType.DMA((ARRIVALS,)),
        ],
        compiler_params=pltpu.CompilerParams(
            collective_id=0, has_side_effects=True, vmem_limit_bytes=44 * 1024 * 1024
        ),
    )(*(pltpu.with_memory_space_constraint(array, pltpu.HBM) for array in operands))
    return (jnp.transpose(mixed, (1, 0, 2)), jnp.transpose(logs, (2, 0, 1)))


def solution(mesh):
    in_specs = (
        P(("sp", "tp"), None, None),
        P(),
        P(None, "sp", "tp"),
        P(None, "sp", "tp"),
        P(None, "sp", "tp"),
        P("tp", "sp"),
    )
    out_specs = (P(("sp", "tp"), None, None), P("sp", None, "tp"))
    return jax.shard_map(shards, mesh=mesh, in_specs=in_specs, out_specs=out_specs, check_vma=False)
```

```python
import functools
import math

import jax
import jax.numpy as jnp
from jax import lax
from jax.experimental import pallas as pl
from jax.experimental.pallas import tpu as pltpu
from jax.sharding import PartitionSpec as P

GROUPS = 3
HEADS = 8
HEAD_WIDTH = 128
STEPS = 24
DILATION_MIDDLE = 4
DILATION_WIDE = 16
WIDTH = 2048
BATCH = 6
SHARE = BATCH // 2
ROWS = 512
AHEAD = (1, 1, 3)
BLOCK = 128
BLOCKS = ROWS // BLOCK
WINDOW = tuple((ahead + 1) * BLOCK for ahead in AHEAD)
KEYS = sum(WINDOW)
PIECE = 64
COLUMNS = 10 * HEAD_WIDTH
UNITS = ((0, 5 * HEAD_WIDTH), (5 * HEAD_WIDTH, 10 * HEAD_WIDTH))
ABSENT = -1e30
ORDER = (
    "t00", "O0", "G0", "t01", "t02", "R0", "G1", "G2", "Op0", "Oa0", "Zm00", "Zp00", "up00",
    "dn00", "Rm0", "Rp0", "Ya00", "g0", "up01", "dn01", "Zmp0", "Zpp0", "Yp00", "Zma0",
    "Zpa0", "Yam0", "O1", "up02", "dn02", "g1", "Rf0", "Yap0", "dn10", "fu0", "R1", "Of0",
    "g2", "Zm01", "Zp01", "Oa1", "Ypm0", "up10", "dn11", "Yaf0", "Ypp0", "Rm1", "fu1", "Rp1",
    "fd0", "Zmf0", "Zpf0", "Op1", "Ya01", "Ypf0", "fu2", "dn12", "Zma1", "Zpa1", "Yp01",
    "Rf1", "Yam1", "up11", "fd1", "Of1", "Yap1", "Zmp1", "Zpp1", "Ypm1", "W0", "o0", "K0",
    "up12", "fd2", "Ypp1", "Yaf1", "Zmf1", "Zpf1", "Km", "Ypf1", "Kp", "K2", "oum", "odm",
    "W1", "N", "Q",
)
Y_CUT = (16, 64)
Z_CUT = (48, 48)

epsilon = 1e-06
MESH = pl.DeviceIdType.MESH


def rms_normed(widened, gain):
    scaled = widened * lax.rsqrt(jnp.mean(widened * widened, axis=-1, keepdims=True) + epsilon)
    return (scaled * gain).astype(jnp.bfloat16)


def dot(a, b):
    return lax.dot_general(a, b, (((1,), (0,)), ((), ())), preferred_element_type=jnp.float32)


def dot_t(a, b):
    return lax.dot_general(a, b, (((1,), (1,)), ((), ())), preferred_element_type=jnp.float32)


def kernel(
    tokens, gain, w_query, w_key, w_value, w_out, out, logs,
    raw, gains, gift, toks, weights, whole_out, queries, near, middle, wide, bias,
    combined, arrived, log_rows, both_logs, own_sem, send_sem, recv_sem,
):
    s, x = lax.axis_index("sp"), lax.axis_index("tp")
    core, chip = lax.rem(s, 2), lax.div(s, 2)
    y, z = lax.rem(chip, 4), lax.div(chip, 4)

    def turn(value, by):
        return lax.rem(value + (by + 4), 4)

    def spot(y_at, z_at, core_at):
        return (z_at * 4 + y_at) * 2 + core_at

    zp, zm, xp, xm = (turn(v, d) for v in (z, x) for d in (1, -1))
    line = lax.rem(y, 2)
    pair_y, apart_y = y + 1 - 2 * line, turn(y, 2 * line - 1)
    share = lax.rem(lax.div(y + 1, 2), 2)
    other = 1 - core
    partner = (spot(y, z, other), x)
    z_plus, z_minus = (spot(y, zp, core), x), (spot(y, zm, core), x)
    x_plus, x_minus = (s, xp), (s, xm)
    upper = lax.div(y, 2)
    later = (spot(3 - y, turn(z, upper), core), x)
    head = 2 * x + core

    crowd = []
    for flip_line in (0, 1):
        for flip_core in (0, 1):
            for step in range(4):
                if flip_line or flip_core or step:
                    y_at = pair_y if flip_line else y
                    core_at = other if flip_core else core
                    crowd.append((flip_line, flip_core, step, (spot(y_at, z, core_at), turn(x, step))))
    y_pair, y_apart = (spot(pair_y, z, core), x), (spot(apart_y, z, core), x)
    greeted = [partner, x_plus, x_minus, y_pair, y_apart, z_plus, z_minus]

    barrier = pltpu.get_barrier_semaphore()
    for device in greeted:
        pl.semaphore_signal(barrier, inc=1, device_id=device, device_id_type=MESH)

    counts, opened = [0], [0]

    def tiles_of(ref):
        return math.prod(ref.shape) * ref.dtype.itemsize // 4096

    def shape_of(count):
        for across_at in range(10, 0, -1):
            if count % across_at == 0 and count // across_at <= WIDTH // 16:
                return count // across_at, across_at
        return None

    def extent(count):
        down, over = shape_of(count)
        return weights.at[: down * 16, : over * HEAD_WIDTH]

    class Transfer:
        def __init__(self):
            self.index = opened[0]
            opened[0] += 1
            self.count = 0

        def begin(self, src, dst, device):
            count = tiles_of(src)
            if counts[-1] >= 520 and shape_of(counts[-1]):
                counts.append(0)
            counts[-1] += count
            self.count += count
            pltpu.make_async_remote_copy(
                src_ref=src, dst_ref=dst, send_sem=send_sem.at[len(counts) - 1],
                recv_sem=recv_sem.at[self.index], device_id=device, device_id_type=MESH,
            ).start()

        def arrive(self):
            self.done = True
            whole = extent(self.count)
            pltpu.make_async_copy(whole, whole, recv_sem.at[self.index]).wait()

    def send(src, dst, device):
        transfer = Transfer()
        transfer.begin(src, dst, device)
        return transfer

    def weight_rows(s_at, unit, first=0, count=PIECE):
        left, right = UNITS[unit]
        return weights.at[pl.ds(pl.multiple_of(s_at * PIECE + first, 16), count), left:right]

    def token_rows(line_at, core_at, x_at, b):
        return toks.at[x_at, b, line_at * 2 + core_at]

    take_tokens = pltpu.make_async_copy(tokens, raw, own_sem.at[0])
    take_gain = pltpu.make_async_copy(gain, gains, own_sem.at[1])
    take_tokens.start()
    take_gain.start()
    parts = [(w, group) for group in (2, 1) for w in (w_key, w_value)] + [(w_out, None)]
    parts += [(w_key, 0), (w_value, 0)] + [(w_query, group) for group in (2, 1, 0)]
    rows = pl.ds(pl.multiple_of(s * PIECE, PIECE), PIECE)

    def part_of(index, core_at):
        w, group = parts[index]
        lanes = pl.ds(pl.multiple_of(core_at * HEAD_WIDTH, HEAD_WIDTH), HEAD_WIDTH)
        src = w.at[:, lanes] if group is None else w.at[group, :, lanes]
        return src, weights.at[rows, index * HEAD_WIDTH : (index + 1) * HEAD_WIDTH]

    for index in range(10):
        pltpu.make_async_copy(*part_of(index, core), own_sem.at[2 + index // 5]).start()

    def normed(b):
        return rms_normed(raw[b].astype(jnp.float32), gains[...])

    take_tokens.wait()
    take_gain.wait()
    for b in range(SHARE):
        toks[x, b, line * 2 + core] = normed(share * SHARE + b)
    for b in range(SHARE):
        gift[b] = normed((1 - share) * SHARE + b)

    pl.semaphore_wait(barrier, len(greeted))

    swap = []
    for unit in (0, 1):
        swap.append(Transfer())
        for index in range(5 * unit, 5 * unit + 5):
            src, dst = part_of(index, other)
            swap[unit].begin(src, dst, partner)

    class Ring:
        def __init__(self, rows_of, first, second, names, cut):
            self.rows_of, self.first, self.second, self.cut = rows_of, first, second, cut
            self.names = names
            rows = rows_of(0)
            to_second, to_first = send(rows, rows, second), send(rows, rows, first)
            along_y = names[0] == "pair"
            self.from_first = to_first if along_y else to_second
            self.from_second = to_second if along_y else to_first
            self.on = Transfer()

        def pass_first(self):
            self.from_first.arrive()
            if self.cut < PIECE:
                rows = self.rows_of(self.names[0], self.cut, PIECE - self.cut)
                self.on.begin(rows, rows, self.second)

        def pass_second(self):
            self.from_second.arrive()
            if self.cut > 0:
                rows = self.rows_of(self.names[1], 0, self.cut)
                self.on.begin(rows, rows, self.first)

        def far(self):
            self.on.arrive()

    ys = {0: y, "pair": pair_y, "apart": apart_y, "far": turn(y, 2)}
    zs = {0: z, -1: zm, 1: zp, 2: turn(z, 2)}

    def y_ring(dz, core_at, unit):
        return Ring(
            lambda step, *cut: weight_rows(spot(ys[step], zs[dz], core_at), unit, *cut),
            y_pair, y_apart, ("pair", "apart"), Y_CUT[unit],
        )

    def z_ring(dy, core_at, unit):
        return Ring(
            lambda step, *cut: weight_rows(spot(ys[dy], zs[step], core_at), unit, *cut),
            z_minus, z_plus, (-1, 1), Z_CUT[unit],
        )

    events = {}

    across = {step: Transfer() for step in (0, -1, 1, 2)}
    lines = (line, 1 - line)
    give, up, down, far_up, far_down = {}, {}, {}, {}, {}

    def cross(step, which, b):
        rows = token_rows(lines[which], core, turn(x, step), b)
        across[step].begin(rows, rows, partner)

    def launch(which, b):
        if which == 1:
            give[b].arrive()
        rows = token_rows(lines[which], core, x, b)
        up[which, b] = send(rows, rows, x_plus)
        down[which, b] = send(rows, rows, x_minus)
        cross(0, which, b)

    def onward(which, step, b):
        (up if step == -1 else down)[which, b].arrive()
        rows = token_rows(lines[which], core, turn(x, step), b)
        if (which, step) == (0, -1):
            far_up[b] = send(rows, rows, x_plus)
        if (which, step) == (1, 1):
            far_down[b] = send(rows, rows, x_minus)
        cross(step, which, b)

    def arrive_far(which, b):
        (far_up, far_down)[which][b].arrive()
        cross(2, which, b)

    def present(b):
        give[b] = send(gift.at[b], token_rows(line, core, x, b), y_pair)

    for b in range(SHARE):
        events[f"G{b}"] = functools.partial(present, b)
        for which in (0, 1):
            events[f"t0{b}" if which == 0 else f"g{b}"] = functools.partial(launch, which, b)
            events[f"up{which}{b}"] = functools.partial(onward, which, -1, b)
            events[f"dn{which}{b}"] = functools.partial(onward, which, 1, b)
            events[f"fu{b}" if which == 0 else f"fd{b}"] = functools.partial(arrive_far, which, b)

    def weight_events(unit):
        rings = {}

        def event(name):
            def keep(work):
                events[name + str(unit)] = work
            return keep

        def over_z(letter, dy):
            ring = rings["z" + letter] = z_ring(dy, core, unit)
            events[f"Zm{letter}{unit}"], events[f"Zp{letter}{unit}"] = ring.pass_first, ring.pass_second

        def over_y(letter, dz):
            ring = rings["y" + letter] = y_ring(dz, other, unit)
            events[f"Yp{letter}{unit}"], events[f"Ya{letter}{unit}"] = ring.pass_first, ring.pass_second

        @event("O")
        def _():
            whole = weight_rows(s, unit)
            pltpu.make_async_copy(whole, whole, own_sem.at[2 + unit]).wait()
            rings["O"] = y_ring(0, core, unit)
            over_z("0", 0)

        @event("R")
        def _():
            swap[unit].arrive()
            rings["R"] = z_ring(0, other, unit)
            over_y("0", 0)

        @event("Op")
        def _():
            rings["O"].pass_first()
            over_z("p", "pair")

        @event("Oa")
        def _():
            rings["O"].pass_second()
            over_z("a", "apart")

        @event("Of")
        def _():
            rings["O"].far()
            over_z("f", "far")

        @event("Rm")
        def _():
            rings["R"].pass_first()
            over_y("m", -1)

        @event("Rp")
        def _():
            rings["R"].pass_second()
            over_y("p", 1)

        @event("Rf")
        def _():
            rings["R"].far()
            over_y("f", 2)

        @event("W")
        def _():
            for letter in "0paf":
                rings["z" + letter].far()
            for letter in "0mpf":
                rings["y" + letter].far()

    weight_events(0)
    weight_events(1)

    def project(x_at, left, width):
        rows = toks[x_at].reshape(SHARE * BLOCKS * 32, WIDTH)
        return dot(rows, weights[:, left : left + width]).astype(jnp.bfloat16)

    def block_rows(x_at):
        return pl.ds(pl.multiple_of(x_at * 32, 32), 32)

    def lay(found, left, buffer, x_at, ahead):
        part = found[:, left : left + HEAD_WIDTH].reshape(SHARE, BLOCKS, 32, HEAD_WIDTH)
        buffer[:, ahead : ahead + BLOCKS, block_rows(x_at), :] = part

    def keys_of(step):
        x_at = turn(x, step)
        across[step].arrive()
        for place, (keys, group) in enumerate(((wide, 2), (middle, 1))):
            found = project(x_at, place * 2 * HEAD_WIDTH, 2 * HEAD_WIDTH)
            for which in (0, 1):
                lay(found, which * HEAD_WIDTH, keys.at[which], x_at, AHEAD[group])

    halo = []

    def pass_on(keys, group, x_at, share_at):
        ahead = AHEAD[group]
        halo.append(
            send(
                keys.at[:, share_at, BLOCKS:, block_rows(x_at), :],
                keys.at[:, share_at, :ahead, block_rows(x_at), :],
                later,
            )
        )

    def pass_all(step):
        for keys, group in ((wide, 2), (middle, 1)):
            pass_on(keys, group, turn(x, step), slice(None))

    def head_columns(x_at, core_at, half=None):
        lanes = pl.ds(pl.multiple_of((2 * x_at + core_at) * HEAD_WIDTH, HEAD_WIDTH), HEAD_WIDTH)
        if half is None:
            return whole_out.at[:, lanes]
        return whole_out.at[pl.ds(half * (WIDTH // 2), WIDTH // 2), lanes]

    out_swap = Transfer()

    out_way = {}

    def out_event(name):
        def keep(work):
            events[name] = work
        return keep

    def out_cross(rows):
        out_swap.begin(rows, rows, partner)

    @out_event("o0")
    def _():
        out_rows = weights.at[:, 4 * HEAD_WIDTH : 5 * HEAD_WIDTH]
        mine = head_columns(x, core)
        out_way["up"] = send(out_rows, mine, x_plus)
        out_way["down"] = send(out_rows, mine, x_minus)
        out_swap.begin(out_rows, mine, partner)
        lanes = pl.ds(pl.multiple_of(head * HEAD_WIDTH, HEAD_WIDTH), HEAD_WIDTH)
        whole_out[:, lanes] = weights[:, 4 * HEAD_WIDTH : 5 * HEAD_WIDTH]

    @out_event("oum")
    def _():
        out_way["up"].arrive()
        rows = head_columns(xm, core, 0)
        out_way["far_up"] = send(rows, rows, x_plus)
        out_cross(head_columns(xm, core))

    @out_event("odm")
    def _():
        out_way["down"].arrive()
        rows = head_columns(xp, core, 1)
        out_way["far_down"] = send(rows, rows, x_minus)
        out_cross(head_columns(xp, core))

    @out_event("ofu")
    def _():
        out_way["far_up"].arrive()
        out_cross(head_columns(turn(x, 2), core, 0))

    @out_event("ofd")
    def _():
        out_way["far_down"].arrive()
        out_cross(head_columns(turn(x, 2), core, 1))

    near[:, :, 0, :96, :] = jnp.zeros((2, SHARE, 96, HEAD_WIDTH), jnp.bfloat16)
    log_rows[...] = jnp.zeros_like(log_rows)
    left = 0
    for ahead, window, dilation in zip(AHEAD, WINDOW, (1, DILATION_MIDDLE, DILATION_WIDE)):
        query_at = lax.broadcasted_iota(jnp.int32, (BLOCK, window), 0)
        key_at = lax.broadcasted_iota(jnp.int32, (BLOCK, window), 1)
        lag = query_at + ahead * BLOCK - key_at
        allowed = (lag >= 0) & (lag <= STEPS * dilation) & ((lag & (dilation - 1)) == 0)
        bias[:, left : left + window] = jnp.where(allowed, jnp.float32(0), jnp.float32(ABSENT))
        left += window

    def keys_near(x_at, carry):
        found = project(x_at, UNITS[1][0], 2 * HEAD_WIDTH)
        for which in (0, 1):
            lay(found, which * HEAD_WIDTH, near.at[which], x_at, AHEAD[0])
        return carry

    def ask(x_at, carry):
        left = UNITS[1][0] + 2 * HEAD_WIDTH
        found = project(x_at, left, 2 * HEAD_WIDTH)
        lay(found, 0, queries.at[2], x_at, 0)
        lay(found, HEAD_WIDTH, queries.at[1], x_at, 0)
        lay(project(x_at, left + 2 * HEAD_WIDTH, HEAD_WIDTH), 0, queries.at[0], x_at, 0)
        return carry

    def early_keys(step):
        keys_of(step)
        pass_all(step)

    for letter, step in (("0", 0), ("m", -1), ("p", 1)):
        events["K" + letter] = functools.partial(early_keys, step)

    @out_event("K2")
    def _():
        keys_of(2)
        for b in range(SHARE):
            for keys, group in ((wide, 2), (middle, 1)):
                pass_on(keys, group, turn(x, 2), pl.ds(b, 1))

    @out_event("N")
    def _():
        lax.fori_loop(0, 4, keys_near, 0)
        halo.append(send(near.at[:, :, BLOCKS, 96:, :], near.at[:, :, 0, 96:, :], later))

    @out_event("Q")
    def _():
        lax.fori_loop(0, 4, ask, 0)

    for name in ORDER:
        events[name]()

    factor = math.log2(math.e) / math.sqrt(HEAD_WIDTH)
    start_at = (z * 2 + upper) * ROWS
    lanes = pl.ds(pl.multiple_of(head * HEAD_WIDTH, HEAD_WIDTH), HEAD_WIDTH)

    def attend(b, block):
        scores, left = [], 0
        for group, keys in enumerate((near, middle, wide)):
            window = WINDOW[group]
            seen = keys[0, b, block : block + AHEAD[group] + 1].reshape(window, HEAD_WIDTH)
            score = dot_t(queries[group, b, block], seen)
            first = start_at + (block - AHEAD[group]) * BLOCK
            hidden = bias[:, left : left + window]
            if block < AHEAD[group]:
                key_at = lax.broadcasted_iota(jnp.int32, (1, window), 1) + first
                hidden = hidden + jnp.where(key_at >= 0, jnp.float32(0), jnp.float32(ABSENT))
            scores.append(score * factor + hidden)
            left += window
        peak = functools.reduce(
            jnp.maximum, [jnp.max(score, axis=1, keepdims=True) for score in scores]
        )
        total, mixed = 0.0, 0.0
        for group, keys in enumerate((near, middle, wide)):
            lifted = jnp.exp2(scores[group] - peak)
            total = total + jnp.sum(lifted, axis=1, keepdims=True)
            seen = keys[1, b, block : block + AHEAD[group] + 1].reshape(WINDOW[group], HEAD_WIDTH)
            mixed = mixed + dot(lifted.astype(jnp.bfloat16), seen)
        combined[b, block * BLOCK : (block + 1) * BLOCK, :] = (mixed / total).astype(jnp.bfloat16)
        log = (peak + jnp.log2(total)) * math.log(2.0)
        log_rows[block, b : b + 1, :] = jnp.transpose(jnp.broadcast_to(log, (BLOCK, BLOCK)))[0:1, :]

    def rows_for(line_at, core_at, x_at):
        return pl.ds(pl.multiple_of(line_at * 256 + core_at * 128 + x_at * 32, 32), 32)

    for b in range(SHARE):
        attend(b, BLOCKS - 1)
    for copy in halo[:6] + halo[12:]:
        copy.arrive()
    exchange = Transfer()
    for b in range(SHARE):
        halo[6 + 2 * b].arrive()
        halo[7 + 2 * b].arrive()
        for block in range(BLOCKS - 1):
            attend(b, block)

        for flip_line, flip_core, step, device in crowd:
            line_at = 1 - line if flip_line else line
            core_at = other if flip_core else core
            exchange.begin(
                combined.at[b, rows_for(line_at, core_at, turn(x, step)), :],
                arrived.at[share * SHARE + b, :, lanes],
                device,
            )
            if step == 0 and b == SHARE - 1:
                exchange.begin(
                    log_rows.at[line_at * 2 + core_at], both_logs.at[core, share], device
                )
        arrived[share * SHARE + b, :, lanes] = combined[b, rows_for(line, core, x), :]
    both_logs[core, share] = log_rows[line * 2 + core]
    events["ofu"]()
    events["ofd"]()
    out_swap.arrive()
    exchange.arrive()

    everything = arrived[...].reshape(192, HEADS * HEAD_WIDTH)
    for tile in range(8):
        part = dot_t(everything, whole_out[tile * 256 : (tile + 1) * 256, :]).astype(jnp.bfloat16)
        out[:, :, tile * 256 : (tile + 1) * 256] = part.reshape(BATCH, 32, 256)
    for core_at in range(2):
        for share_at in range(2):
            for b in range(SHARE):
                logs[share_at * SHARE + b, core_at : core_at + 1, :] = both_logs[core_at, share_at, b : b + 1, :]

    assert opened[0] <= ARRIVALS and len(counts) <= SENDS, (opened, counts)
    for index, count in enumerate(counts):
        whole = extent(count)
        pltpu.make_async_copy(whole, whole, send_sem.at[index]).wait()


ARRIVALS = 106
SENDS = 8


def shards(tokens, norm_gain, w_query, w_key, w_value, w_out):
    bf16, f32 = jnp.bfloat16, jnp.float32
    operands = (
        jnp.transpose(tokens, (1, 0, 2)), norm_gain.reshape(1, WIDTH),
        w_query, w_key, w_value, jnp.transpose(w_out),
    )
    mixed, logs = pl.pallas_call(
        kernel,
        out_shape=(
            jax.ShapeDtypeStruct((BATCH, 32, WIDTH), bf16),
            jax.ShapeDtypeStruct((BATCH, 2, 128), f32),
        ),
        in_specs=[pl.BlockSpec(memory_space=pltpu.HBM)] * 6,
        out_specs=[pl.BlockSpec(memory_space=pltpu.VMEM)] * 2,
        scratch_shapes=[
            pltpu.VMEM((BATCH, 32, WIDTH), bf16),
            pltpu.VMEM((1, WIDTH), f32),
            pltpu.VMEM((SHARE, 32, WIDTH), bf16),
            pltpu.VMEM((4, SHARE, BLOCKS, 32, WIDTH), bf16),
            pltpu.VMEM((WIDTH, COLUMNS), bf16),
            pltpu.VMEM((WIDTH, HEADS * HEAD_WIDTH), bf16),
            pltpu.VMEM((GROUPS, SHARE, BLOCKS, BLOCK, HEAD_WIDTH), bf16),
            pltpu.VMEM((2, SHARE, AHEAD[0] + BLOCKS, BLOCK, HEAD_WIDTH), bf16),
            pltpu.VMEM((2, SHARE, AHEAD[1] + BLOCKS, BLOCK, HEAD_WIDTH), bf16),
            pltpu.VMEM((2, SHARE, AHEAD[2] + BLOCKS, BLOCK, HEAD_WIDTH), bf16),
            pltpu.VMEM((BLOCK, KEYS), f32),
            pltpu.VMEM((SHARE, ROWS, HEAD_WIDTH), bf16),
            pltpu.VMEM((BATCH, 32, HEADS * HEAD_WIDTH), bf16),
            pltpu.VMEM((4, 8, 128), f32),
            pltpu.VMEM((2, 2, 8, 128), f32),
            pltpu.SemaphoreType.DMA((4,)),
            pltpu.SemaphoreType.DMA((SENDS,)),
            pltpu.SemaphoreType.DMA((ARRIVALS,)),
        ],
        compiler_params=pltpu.CompilerParams(
            collective_id=0, has_side_effects=True, vmem_limit_bytes=44 * 1024 * 1024
        ),
    )(*(pltpu.with_memory_space_constraint(array, pltpu.HBM) for array in operands))
    return (jnp.transpose(mixed, (1, 0, 2)), jnp.transpose(logs, (2, 0, 1)))


def solution(mesh):
    in_specs = (
        P(("sp", "tp"), None, None),
        P(),
        P(None, "sp", "tp"),
        P(None, "sp", "tp"),
        P(None, "sp", "tp"),
        P("tp", "sp"),
    )
    out_specs = (P(("sp", "tp"), None, None), P("sp", None, "tp"))
    return jax.shard_map(shards, mesh=mesh, in_specs=in_specs, out_specs=out_specs, check_vma=False)
```
